512 devices in a mesh: sp: 128 (over z, y, core), tp: 4 (over x).
Axes of the slice: x: 4, y: 8, z: 8, core: 2. Of those that a mesh axis runs over, the one named last changes fastest.
Arguments:
- tokens: bfloat16 [32768, 2048], P(('sp', 'tp')), may hold values from -6 to 6
- norm_gain: float32 [2048], replicated, may hold values from 0.1 to 1.9
- ret_query: bfloat16 [2048, 1024], P('sp', 'tp'), may hold values from -0.125 to 0.125
- ret_key: bfloat16 [2048, 1024], P('sp', 'tp'), may hold values from -0.125 to 0.125
- ret_value: bfloat16 [2048, 2048], P('sp', 'tp'), may hold values from -0.125 to 0.125
- log_decay: float32 [8, 32768], P('tp', 'sp'), may hold values from -2 to 0, as said below
- att_query: bfloat16 [2048, 2048], P('sp', 'tp')
- att_key: bfloat16 [2048, 256], P('sp', 'tp')
- att_value: bfloat16 [2048, 256], P('sp', 'tp'), may hold values from -0.125 to 0.125
- sink_logits: float32 [32], P('tp'), may hold values from 3 to 6
- ret_out: bfloat16 [2048, 2048], P('tp', 'sp'), may hold values from -0.125 to 0.125
- att_out: bfloat16 [2048, 2048], P('tp', 'sp'), may hold values from -1 to 1
Outputs:
- mixed: bfloat16 [32768, 2048], P(('sp', 'tp'))
The draws below stay inside these ranges and needn't reach their ends.
Inputs may be any that keep to these rules, and one draw needn't show every extreme that they name: `log_decay`: strictly negative.
All inputs are finite; a program needn't handle non-finite values.
Results may differ from the reference program's by a relative error of at most 0.013.
Values may be sent and summed in bfloat16 or wider, within the bound.
No kernel may reach another device: no remote copies, remote signals or barrier semaphores. Data moves between devices by JAX's collectives and lax.ppermute only.
A program may use at most 128 MiB of HBM per device.

```python
import jax
import jax.numpy as jnp
from jax import lax

D = 2048
RET_HEADS = 8
RETAIN_KEY_SIZE = 128
V_DIM = 256
ASKER_HEADCOUNT = 32
KV_HEADS = 4
HEAD_DIM = 64
WINDOW = 128
BLOCK = 128
TOKENS = 32768
N_TP = 4


def attend_pair(key):
    lookup_matrix = jax.random.normal(jax.random.fold_in(key, 11), (D, KV_HEADS * HEAD_DIM), jnp.float32) * D ** (-0.5)
    query_weight = jax.random.normal(jax.random.fold_in(key, 12), (D, ASKER_HEADCOUNT * HEAD_DIM), jnp.float32) * D ** (-0.5)
    return (query_weight, lookup_matrix)


def draw_att_query(key, part):
    return attend_pair(key)[0].astype(jnp.bfloat16)


def draw_att_key(key, part):
    return attend_pair(key)[1].astype(jnp.bfloat16)


def draw_log_decay(key, part):
    slow_share = 0.5
    picked = jax.random.uniform(jax.random.fold_in(key, 21), (RET_HEADS,))
    fast_rate = jax.random.uniform(jax.random.fold_in(key, 22), (RET_HEADS,), minval=1.0 / 100.0, maxval=1.0 / 30.0)
    slow_rate = jax.random.uniform(jax.random.fold_in(key, 23), (RET_HEADS,), minval=0.2, maxval=0.6) / TOKENS
    speed_numbers = jnp.where(picked < slow_share, slow_rate, fast_rate)
    tempo_numbers = jax.random.uniform(jax.random.fold_in(key, 24), (TOKENS // BLOCK,), minval=0.6, maxval=1.5)
    tempo_numbers = jnp.repeat(tempo_numbers, BLOCK)
    spots = jax.random.randint(jax.random.fold_in(key, 25), (RET_HEADS, 2), 0, TOKENS)
    objective_numbers = jnp.log(jax.random.uniform(jax.random.fold_in(key, 26), (RET_HEADS, 2), minval=0.5, maxval=0.8))
    removed_elements = jnp.arange(TOKENS)[None, None, :] == spots[:, :, None]
    spike_sequence = jnp.sum(jnp.where(removed_elements, objective_numbers[:, :, None], 0.0), axis=1)
    return -speed_numbers[:, None] * tempo_numbers[None, :] + spike_sequence


def shard_levels(own_key, extent, pieces, least, top_value):
    def one(position, shards_of):
        steps = jax.random.uniform(jax.random.fold_in(jax.random.fold_in(own_key, 6), position), (shards_of,), jnp.float32, least / len(pieces), top_value / len(pieces))
        return jnp.repeat(jnp.exp(steps), extent[position] // shards_of).reshape((-1,) + (1,) * (len(extent) - position - 1))

    gain = one(*pieces[0])
    for cut in pieces[1:]:
        gain = gain * one(*cut)
    return gain


def centred(rng, shape, deviation, bound, shards=(), kind=jnp.bfloat16):
    factor_of = shard_levels(rng, shape, shards, -0.22, 0.18) if shards else 1.0
    result = jax.random.normal(rng, shape, jnp.float32) * deviation * factor_of
    return jnp.minimum(jnp.maximum(result, -bound), bound).astype(kind)


def setup_inputs(seed: int = 0) -> dict:
    seeds = jax.random.split(jax.random.key(seed), 13)
    return {
        "tokens": centred(seeds[0], (TOKENS, D), 1.0, 6.0, ((0, 512),)),
        "norm_gain": jnp.clip(1.0 + 0.18 * jax.random.normal(seeds[1], (D,), jnp.float32), 0.1, 1.9),
        "ret_query": centred(seeds[2], (D, RET_HEADS * RETAIN_KEY_SIZE), D ** -0.5, 0.125, ((0, 128), (1, 4))),
        "ret_key": centred(seeds[3], (D, RET_HEADS * RETAIN_KEY_SIZE), D ** -0.5, 0.125, ((0, 128), (1, 4))),
        "ret_value": centred(seeds[4], (D, RET_HEADS * V_DIM), D ** -0.5, 0.125, ((0, 128), (1, 4))),
        "log_decay": draw_log_decay(jax.random.fold_in(seeds[12], 71), 0),
        "att_query": draw_att_query(jax.random.fold_in(seeds[12], 71), 0),
        "att_key": draw_att_key(jax.random.fold_in(seeds[12], 71), 0),
        "att_value": centred(seeds[8], (D, KV_HEADS * HEAD_DIM), D ** -0.5, 0.125, ((0, 128), (1, 4))),
        "sink_logits": jnp.clip(3.0 + 3.0 * jax.random.uniform(seeds[9], (ASKER_HEADCOUNT,), jnp.float32) ** shard_levels(seeds[9], (ASKER_HEADCOUNT,), ((0, 4),), -0.2, 0.2), 3.0, 6.0),
        "ret_out": centred(seeds[10], (RET_HEADS * V_DIM, D), (RET_HEADS * V_DIM) ** -0.5, 0.125, ((0, 4), (1, 128))),
        "att_out": centred(seeds[11], (ASKER_HEADCOUNT * HEAD_DIM, D), (ASKER_HEADCOUNT * HEAD_DIM // 64) ** -0.5, 1.0, ((0, 4), (1, 128))),
    }


epsilon = 1e-05
rope_base = 10000.0
masked_out = -1e+30

def rounded(values):
    return lax.optimization_barrier(values.astype(jnp.bfloat16))

def rotate(values, positions):
    half_dim = values.shape[-1] // 2
    inverse = rope_base ** (-jnp.arange(half_dim, dtype=jnp.float32) / half_dim)
    angles = positions.astype(jnp.float32)[:, None] * inverse[None, :]
    cosine = jnp.cos(angles)[:, None, :]
    sine_part = jnp.sin(angles)[:, None, :]
    first_half = values[..., :half_dim].astype(jnp.float32)
    second_half = values[..., half_dim:].astype(jnp.float32)
    return jnp.concatenate([first_half * cosine - second_half * sine_part, second_half * cosine + first_half * sine_part], axis=-1)

def retain(query, keys, values, log_decay):
    length, head_count, key_depth = query.shape
    value_width = values.shape[-1]
    block_count = length // BLOCK
    q_blocks = query.reshape(block_count, BLOCK, head_count, key_depth).astype(jnp.float32)
    k_blocks = keys.reshape(block_count, BLOCK, head_count, key_depth).astype(jnp.float32)
    v_blocks = values.reshape(block_count, BLOCK, head_count, value_width).astype(jnp.float32)
    running = jnp.cumsum(log_decay.reshape(head_count, block_count, BLOCK), axis=-1)
    closing = running[:, :, -1:]
    within = running[:, :, :, None] - running[:, :, None, :]
    causal_mask = jnp.arange(BLOCK)[:, None] >= jnp.arange(BLOCK)[None, :]
    weighting = jnp.where(causal_mask, jnp.exp(jnp.minimum(within, 0.0)), 0.0)
    scores = jnp.einsum('nihd,njhd->hnij', q_blocks, k_blocks) * weighting
    in_block = jnp.einsum('hnij,njhv->nihv', rounded(scores).astype(jnp.float32), v_blocks)
    key_fade = rounded(k_blocks * jnp.exp(closing - running).transpose(1, 2, 0)[..., None])
    contrib = jnp.einsum('njhd,njhv->nhdv', key_fade.astype(jnp.float32), v_blocks)
    block_fade = jnp.exp(closing[:, :, 0]).T

    def advance(carried, entry_pair):
        addend, factor = entry_pair
        return (carried * factor[:, None, None] + addend, carried)
    _, before = lax.scan(advance, jnp.zeros((head_count, key_depth, value_width), jnp.float32), (contrib, block_fade))
    query_fade = rounded(q_blocks * jnp.exp(running).transpose(1, 2, 0)[..., None])
    carried_term = jnp.einsum('nihd,nhdv->nihv', query_fade.astype(jnp.float32), before, precision=lax.Precision.HIGHEST)
    final_product = in_block + carried_term
    final_product = final_product * lax.rsqrt(lax.optimization_barrier(jnp.mean(final_product * final_product, axis=-1, keepdims=True)) + epsilon)
    return final_product.reshape(length, head_count * value_width).astype(jnp.bfloat16)

def one_group(group_entry):
    queries, keys, values, sink_row = group_entry
    length = keys.shape[0]
    group_size = queries.shape[1]
    block_count = length // WINDOW
    zeroed = jnp.zeros((WINDOW, HEAD_DIM), jnp.bfloat16)
    key_ext = jnp.concatenate([zeroed, keys], axis=0).reshape(block_count + 1, WINDOW, HEAD_DIM)
    value_ext = jnp.concatenate([zeroed, values], axis=0).reshape(block_count + 1, WINDOW, HEAD_DIM)
    keys_pair = jnp.concatenate([key_ext[:-1], key_ext[1:]], axis=1).astype(jnp.float32)
    values_pair = jnp.concatenate([value_ext[:-1], value_ext[1:]], axis=1).astype(jnp.float32)
    q_blocks = queries.reshape(block_count, WINDOW, group_size, HEAD_DIM).astype(jnp.float32)
    scores = jnp.einsum('nigd,njd->ngij', q_blocks, keys_pair) * HEAD_DIM ** (-0.5)
    query_pos = (jnp.arange(block_count) * WINDOW)[:, None] + jnp.arange(WINDOW)[None, :]
    key_pos = (jnp.arange(block_count) * WINDOW - WINDOW)[:, None] + jnp.arange(2 * WINDOW)[None, :]
    allowed = (key_pos[:, None, :] >= 0) & (key_pos[:, None, :] <= query_pos[:, :, None]) & (query_pos[:, :, None] - key_pos[:, None, :] < WINDOW)
    scores = jnp.where(allowed[:, None], scores, masked_out)
    sink_logit = sink_row[None, :, None]
    highest = jnp.maximum(lax.optimization_barrier(jnp.max(scores, axis=-1)), sink_logit)
    lifted = jnp.exp(scores - highest[..., None])
    denominator = lax.optimization_barrier(jnp.sum(lifted, axis=-1)) + jnp.exp(sink_logit - highest)
    attn_weights = rounded(lifted / denominator[..., None])
    final_product = jnp.einsum('ngij,njd->nigd', attn_weights.astype(jnp.float32), values_pair)
    return final_product.reshape(length, group_size * HEAD_DIM).astype(jnp.bfloat16)

def reference(tokens, norm_gain, ret_query, ret_key, ret_value, log_decay, att_query, att_key, att_value, sink_logits, ret_out, att_out):
    tok_float = tokens.astype(jnp.float32)
    normed = (tok_float * lax.rsqrt(lax.optimization_barrier(jnp.mean(tok_float * tok_float, axis=-1, keepdims=True)) + epsilon) * norm_gain).astype(jnp.bfloat16)

    def project(weight):
        return jnp.dot(normed, weight, preferred_element_type=jnp.float32).astype(jnp.bfloat16)
    positions = jnp.arange(TOKENS, dtype=jnp.int32)
    query_ret = rotate(project(ret_query).reshape(TOKENS, RET_HEADS, RETAIN_KEY_SIZE), positions).astype(jnp.bfloat16)
    key_ret = (rotate(project(ret_key).reshape(TOKENS, RET_HEADS, RETAIN_KEY_SIZE), positions) * RETAIN_KEY_SIZE ** (-0.5)).astype(jnp.bfloat16)
    value_ret = project(ret_value).reshape(TOKENS, RET_HEADS, V_DIM)
    ret_mix = retain(query_ret, key_ret, value_ret, log_decay)
    group_size = ASKER_HEADCOUNT // KV_HEADS
    query_att = project(att_query).reshape(TOKENS, KV_HEADS, group_size, HEAD_DIM).transpose(1, 0, 2, 3)
    key_att = project(att_key).reshape(TOKENS, KV_HEADS, HEAD_DIM).transpose(1, 0, 2)
    value_att = project(att_value).reshape(TOKENS, KV_HEADS, HEAD_DIM).transpose(1, 0, 2)
    att_mix = lax.map(one_group, (query_att, key_att, value_att, sink_logits.reshape(KV_HEADS, group_size)))
    att_mix = att_mix.transpose(1, 0, 2).reshape(TOKENS, ASKER_HEADCOUNT * HEAD_DIM)
    ret_share = RET_HEADS * V_DIM // N_TP
    att_share = ASKER_HEADCOUNT * HEAD_DIM // N_TP
    summed = jnp.zeros((TOKENS, D), jnp.float32)
    for group_index in range(N_TP):
        ret_cols = slice(group_index * ret_share, (group_index + 1) * ret_share)
        att_cols = slice(group_index * att_share, (group_index + 1) * att_share)
        partial_total_sum = jnp.dot(ret_mix[:, ret_cols], ret_out[ret_cols], preferred_element_type=jnp.float32)
        partial_total_sum = partial_total_sum + jnp.dot(att_mix[:, att_cols], att_out[att_cols], preferred_element_type=jnp.float32)
        summed = summed + rounded(partial_total_sum).astype(jnp.float32)
    return summed.astype(jnp.bfloat16)
```

```python
import jax
import jax.numpy as jnp
from jax import lax
from jax.experimental import pallas as pl
from jax.sharding import Mesh
from jax.sharding import PartitionSpec as P

RETAIN_KEY_SIZE = 128
V_DIM = 256
HEAD_DIM = 64
WINDOW = 128
BLOCK = 128
SP = ("sp_0", "sp_1", "sp_2")
SP_TP = ("sp_0", "sp_1", "sp_2", "tp")


epsilon = 1e-05
rope_base = 10000.0
masked_out = -1e30


def shifted(value, axis, steps):
    count = lax.axis_size(axis)
    initial, last = (max(0, -steps), min(count, count - steps))
    return lax.ppermute(value, axis, [(source, source + steps) for source in range(initial, last)])


def gather_turned(arrays, axis, dims):
    turned = [jnp.moveaxis(a, dim, 0) for a, dim in zip(arrays, dims)]
    widths = [t[0].size for t in turned]
    both = jnp.concatenate([t.reshape(-1, w) for t, w in zip(turned, widths)], axis=1)
    whole = lax.all_gather(both, axis, axis=0, tiled=True)
    tiles = jnp.split(whole, [sum(widths[:k]) for k in range(1, len(widths))], axis=1)
    return tuple(
        (
            jnp.moveaxis(b.reshape(-1, *t.shape[1:]), 0, dim)
            for b, t, dim in zip(tiles, turned, dims)
        )
    )


def cut_along(value, dim, size):
    before, after = (value.shape[:dim], value.shape[dim + 1 :])
    return jnp.moveaxis(value.reshape(*before, size, -1, *after), dim, 0)


def sent_and_summed(value, axis, dim):
    tiles = cut_along(value, dim, lax.axis_size(axis))
    arrived = lax.all_to_all(tiles, axis, split_axis=0, concat_axis=0, tiled=True)
    return arrived.astype(jnp.float32).sum(axis=0)


def rotate(values, positions):
    half_dim = values.shape[-1] // 2
    inverse = rope_base ** (-jnp.arange(half_dim, dtype=jnp.float32) / half_dim)
    angles = positions.astype(jnp.float32)[:, None] * inverse[None, :]
    cosine = jnp.cos(angles)[:, None, :]
    sine_part = jnp.sin(angles)[:, None, :]
    first_half = values[..., :half_dim].astype(jnp.float32)
    second_half = values[..., half_dim:].astype(jnp.float32)
    return jnp.concatenate(
        [
            first_half * cosine - second_half * sine_part,
            second_half * cosine + first_half * sine_part,
        ],
        axis=-1,
    )


ZY = ("sp_0", "sp_1")
CORE = "sp_2"


def core_swap(value):
    return lax.ppermute(value, CORE, [(0, 1), (1, 0)])


def in_core_order(own, other, axis):
    first = lax.axis_index(CORE) == 0
    return jnp.concatenate(
        [jnp.where(first, own, other), jnp.where(first, other, own)], axis=axis
    )


def prefix_body(parts_ref, out_ref):
    count = parts_ref.shape[0]
    carried = jnp.zeros(out_ref.shape[1:], jnp.float32)
    for k in range(count):
        out_ref[k] = carried
        carried = carried * jnp.exp(parts_ref[k, 2:3]) + parts_ref[k, :2]


def state_before(total, log_total):
    count = lax.axis_size(ZY)
    slices = total.reshape(count, 2, V_DIM)
    marks = jnp.broadcast_to(log_total, (count, 1, V_DIM))
    sent = jnp.concatenate([slices, marks], axis=1)
    arrived = lax.all_to_all(sent, ZY, 0, 0, tiled=True)
    prefix = pl.pallas_call(
        prefix_body, out_shape=jax.ShapeDtypeStruct((count, 2, V_DIM), jnp.float32)
    )(arrived)
    return lax.all_to_all(prefix, ZY, 0, 0, tiled=True).reshape(RETAIN_KEY_SIZE, V_DIM)


def weight_of_head(ret_key, ret_value):
    devices = lax.axis_size(SP)
    rows = ret_key.shape[0]
    heads = lax.axis_size(CORE)
    keys = ret_key.reshape(rows, heads, RETAIN_KEY_SIZE)
    values = ret_value.reshape(rows, heads, V_DIM)
    both = jnp.moveaxis(jnp.concatenate([keys, values], axis=2), 1, 0)
    sent = jnp.broadcast_to(both[None], (devices // heads, *both.shape)).reshape(
        devices, rows, -1
    )
    arrived = lax.all_to_all(sent, SP, 0, 0, tiled=True)
    return arrived.reshape(devices * rows, -1)


def chain_of_head(kv, log_decay, anchor):
    length = kv.shape[0]
    blocks = length // BLOCK
    positions = anchor + jnp.arange(length, dtype=jnp.int32)
    keys = (
        rotate(kv[:, None, :RETAIN_KEY_SIZE], positions)[:, 0] * RETAIN_KEY_SIZE ** (-0.5)
    ).astype(jnp.bfloat16)
    values = kv[:, RETAIN_KEY_SIZE:]
    running = jnp.cumsum(log_decay.reshape(blocks, BLOCK), axis=-1)
    closing = running[:, -1]
    faded = (
        keys.reshape(blocks, BLOCK, -1).astype(jnp.float32)
        * jnp.exp(closing[:, None] - running)[..., None]
    ).astype(jnp.bfloat16)
    contrib = jnp.einsum(
        "njd,njv->ndv", faded, values.reshape(blocks, BLOCK, -1), preferred_element_type=jnp.float32
    )
    total = contrib[0]
    for n in range(1, blocks):
        total = total * jnp.exp(closing[n]) + contrib[n]
    state = state_before(total, jnp.sum(closing))
    before = []
    for n in range(blocks):
        before.append(state)
        state = state * jnp.exp(closing[n]) + contrib[n]
    return keys, values, jnp.stack(before)


def retention_path(query_ret, key_ret, value_ret, log_decay, before):
    tok_count, heads_here = (query_ret.shape[0], query_ret.shape[1])
    blocks = tok_count // BLOCK
    q_blocks = query_ret.reshape(blocks, BLOCK, heads_here, RETAIN_KEY_SIZE)
    k_blocks = key_ret.reshape(heads_here, blocks, BLOCK, RETAIN_KEY_SIZE)
    v_blocks = value_ret.reshape(heads_here, blocks, BLOCK, V_DIM)
    running = jnp.cumsum(log_decay.reshape(heads_here, blocks, BLOCK), axis=-1)
    within = running[:, :, :, None] - running[:, :, None, :]
    causal_mask = jnp.arange(BLOCK)[:, None] >= jnp.arange(BLOCK)[None, :]
    weighting = jnp.where(causal_mask, jnp.exp(jnp.minimum(within, 0.0)), 0.0)
    scores = (
        jnp.einsum("nihd,hnjd->hnij", q_blocks, k_blocks, preferred_element_type=jnp.float32)
        * weighting
    )
    in_block = jnp.einsum(
        "hnij,hnjv->nihv", scores.astype(jnp.bfloat16), v_blocks, preferred_element_type=jnp.float32
    )
    query_fade = (
        q_blocks.astype(jnp.float32) * jnp.exp(running).transpose(1, 2, 0)[..., None]
    ).astype(jnp.bfloat16)
    carried_term = jnp.einsum("nihd,hndv->nihv", query_fade.astype(jnp.float32), before)
    final_product = in_block + carried_term
    final_product = final_product * lax.rsqrt(
        jnp.mean(final_product * final_product, axis=-1, keepdims=True) + epsilon
    )
    return final_product.reshape(tok_count, heads_here * V_DIM).astype(jnp.bfloat16)


def attention_path(query_att, key_att, value_att, sink_logits, anchor):
    tok_count = query_att.shape[0]
    kv_here = key_att.shape[1] // HEAD_DIM
    group_size = query_att.shape[1] // (kv_here * HEAD_DIM)
    stacked = jnp.concatenate([key_att, value_att], axis=1)
    window_rim = shifted(stacked[tok_count - WINDOW :], SP, 1)
    blocks = tok_count // WINDOW
    extended = jnp.concatenate([window_rim, stacked], axis=0).reshape(
        blocks + 1, WINDOW, 2, kv_here, HEAD_DIM
    )
    paired = jnp.concatenate([extended[:-1], extended[1:]], axis=1)
    keys_pair = paired[:, :, 0]
    values_pair = paired[:, :, 1]
    q_blocks = query_att.reshape(blocks, WINDOW, kv_here, group_size, HEAD_DIM)
    scores = jnp.einsum(
        "nihgd,njhd->nhgij", q_blocks, keys_pair, preferred_element_type=jnp.float32
    ) * HEAD_DIM ** (-0.5)
    query_pos = anchor + (jnp.arange(blocks) * WINDOW)[:, None] + jnp.arange(WINDOW)[None, :]
    key_pos = (
        anchor + (jnp.arange(blocks) * WINDOW - WINDOW)[:, None] + jnp.arange(2 * WINDOW)[None, :]
    )
    allowed = (
        (key_pos[:, None, :] >= 0)
        & (key_pos[:, None, :] <= query_pos[:, :, None])
        & (query_pos[:, :, None] - key_pos[:, None, :] < WINDOW)
    )
    scores = jnp.where(allowed[:, None, None], scores, masked_out)
    sink_logit = sink_logits.reshape(kv_here, group_size)[None, :, :, None]
    highest = jnp.maximum(jnp.max(scores, axis=-1), sink_logit)
    lifted = jnp.exp(scores - highest[..., None])
    denominator = jnp.sum(lifted, axis=-1) + jnp.exp(sink_logit - highest)
    attn_weights = (lifted / denominator[..., None]).astype(jnp.bfloat16)
    final_product = jnp.einsum(
        "nhgij,njhd->nihgd", attn_weights, values_pair, preferred_element_type=jnp.float32
    )
    return final_product.reshape(tok_count, kv_here * group_size * HEAD_DIM).astype(jnp.bfloat16)


def on_device(
    tokens,
    norm_gain,
    ret_query,
    ret_key,
    ret_value,
    log_decay,
    att_query,
    att_key,
    att_value,
    sink_logits,
    ret_out,
    att_out,
):
    core = lax.axis_index(CORE)
    tok_float = tokens.astype(jnp.float32)
    normed = (
        tok_float
        * lax.rsqrt(jnp.mean(tok_float * tok_float, axis=-1, keepdims=True) + epsilon)
        * norm_gain
    ).astype(jnp.bfloat16)
    weights = (ret_query, att_query, att_key, att_value)
    widths = [weight.shape[1] for weight in weights]
    points = [sum(widths[:index]) for index in range(1, len(widths))]
    every_weight = gather_turned(
        (ret_query, att_query, att_key, att_value, ret_out, att_out), SP, (0, 0, 0, 0, 1, 1)
    )
    gathered = every_weight[:4]
    out_whole = every_weight[4:]

    pair = jnp.stack([normed, core_swap(normed)])
    size = lax.axis_size("tp")
    arrived = lax.all_to_all(
        jnp.broadcast_to(pair[None], (size, *pair.shape)), "tp", 0, 0, tiled=True
    )
    chip_rows = arrived.reshape(-1, arrived.shape[-1])
    head_weight = weight_of_head(ret_key, ret_value)
    kv = jnp.dot(chip_rows, head_weight, preferred_element_type=jnp.float32).astype(jnp.bfloat16)
    kv = jnp.moveaxis(kv.reshape(size, 2, -1, kv.shape[-1]), 1, 0)
    kv = kv.reshape(2, -1, kv.shape[-1])
    decay_other = core_swap(log_decay)
    own_head = lax.dynamic_index_in_dim(log_decay, core, 0, keepdims=False)
    other_half = lax.dynamic_index_in_dim(decay_other, core, 0, keepdims=False)
    tok_count = kv.shape[1]
    anchor = lax.axis_index(SP) * tok_count
    chip_anchor = lax.axis_index(ZY) * (2 * tok_count)
    keys, values, before = chain_of_head(
        in_core_order(kv[0], kv[1], 0), in_core_order(own_head, other_half, 0), chip_anchor
    )

    def heads_of_own_rows(value):
        halves = value.reshape(2, value.shape[0] // 2, *value.shape[1:])
        mine = lax.dynamic_index_in_dim(halves, core, 0, keepdims=False)
        theirs = lax.dynamic_index_in_dim(halves, 1 - core, 0, keepdims=False)
        return in_core_order(mine[None], core_swap(theirs)[None], 0)

    key_ret = heads_of_own_rows(keys)
    value_ret = heads_of_own_rows(values)
    before = heads_of_own_rows(before)

    joined = jnp.concatenate(gathered, axis=1)
    own_rows = arrived.reshape(size, 2, -1, arrived.shape[-1])[:, 0].reshape(tok_count, -1)
    projected = jnp.dot(own_rows, joined, preferred_element_type=jnp.float32).astype(jnp.bfloat16)
    sections = jnp.split(projected, points, axis=1)
    positions = anchor + jnp.arange(tok_count, dtype=jnp.int32)
    query_ret = rotate(sections[0].reshape(tok_count, -1, RETAIN_KEY_SIZE), positions).astype(
        jnp.bfloat16
    )
    ret_mix = retention_path(query_ret, key_ret, value_ret, log_decay, before)
    att_mix = attention_path(sections[1], sections[2], sections[3], sink_logits, anchor)
    mixed = sent_and_summed(
        (
            jnp.dot(ret_mix, out_whole[0], preferred_element_type=jnp.float32)
            + jnp.dot(att_mix, out_whole[1], preferred_element_type=jnp.float32)
        ).astype(jnp.bfloat16),
        "tp",
        0,
    )
    return mixed.astype(jnp.bfloat16)


def solution(mesh):
    split = Mesh(mesh.devices.reshape(8, 8, 2, mesh.shape["tp"]), ("sp_0", "sp_1", "sp_2", "tp"))
    placed = (
        P(SP_TP, None),
        P(),
        P(SP, "tp"),
        P(SP, "tp"),
        P(SP, "tp"),
        P("tp", SP),
        P(SP, "tp"),
        P(SP, "tp"),
        P(SP, "tp"),
        P("tp"),
        P("tp", SP),
        P("tp", SP),
    )
    return jax.shard_map(
        on_device, mesh=split, in_specs=placed, out_specs=P(SP_TP, None), check_vma=False
    )
```

```python
import jax
import jax.numpy as jnp
from jax import lax
from jax.experimental import pallas as pl
from jax.sharding import Mesh
from jax.sharding import PartitionSpec as P

RETAIN_KEY_SIZE = 128
V_DIM = 256
HEAD_DIM = 64
WINDOW = 128
BLOCK = 128
SP = ("sp_0", "sp_1", "sp_2")
SP_TP = ("sp_0", "sp_1", "sp_2", "tp")


epsilon = 1e-05
rope_base = 10000.0
masked_out = -1e30


def shifted(value, axis, steps):
    count = lax.axis_size(axis)
    initial, last = (max(0, -steps), min(count, count - steps))
    return lax.ppermute(value, axis, [(source, source + steps) for source in range(initial, last)])


def from_everyone(value, axis):
    size = lax.axis_size(axis)
    return lax.all_to_all(
        jnp.broadcast_to(value[None], (size, *value.shape)), axis, 0, 0, tiled=True
    )


def cut_along(value, dim, size):
    before, after = (value.shape[:dim], value.shape[dim + 1 :])
    return jnp.moveaxis(value.reshape(*before, size, -1, *after), dim, 0)


def sent_and_summed(value, axis, dim):
    tiles = cut_along(value, dim, lax.axis_size(axis))
    arrived = lax.all_to_all(tiles, axis, split_axis=0, concat_axis=0, tiled=True)
    return arrived.astype(jnp.float32).sum(axis=0)


def rotate(values, positions):
    half_dim = values.shape[-1] // 2
    inverse = rope_base ** (-jnp.arange(half_dim, dtype=jnp.float32) / half_dim)
    angles = positions.astype(jnp.float32)[:, None] * inverse[None, :]
    cosine = jnp.cos(angles)[:, None, :]
    sine_part = jnp.sin(angles)[:, None, :]
    first_half = values[..., :half_dim].astype(jnp.float32)
    second_half = values[..., half_dim:].astype(jnp.float32)
    return jnp.concatenate(
        [
            first_half * cosine - second_half * sine_part,
            second_half * cosine + first_half * sine_part,
        ],
        axis=-1,
    )


ZY = ("sp_0", "sp_1")
CORE = "sp_2"


def core_swap(value):
    return lax.ppermute(value, CORE, [(0, 1), (1, 0)])


def in_core_order(own, other, axis):
    first = lax.axis_index(CORE) == 0
    return jnp.concatenate(
        [jnp.where(first, own, other), jnp.where(first, other, own)], axis=axis
    )


def prefix_body(parts_ref, out_ref):
    count = parts_ref.shape[0]
    carried = jnp.zeros(out_ref.shape[1:], jnp.float32)
    for k in range(count):
        out_ref[k] = carried
        carried = carried * jnp.exp(parts_ref[k, 2:3]) + parts_ref[k, :2]


def state_before(total, log_total):
    count = lax.axis_size(ZY)
    slices = total.reshape(count, 2, V_DIM)
    marks = jnp.broadcast_to(log_total, (count, 1, V_DIM))
    sent = jnp.concatenate([slices, marks], axis=1)
    arrived = lax.all_to_all(sent, ZY, 0, 0, tiled=True)
    prefix = pl.pallas_call(
        prefix_body, out_shape=jax.ShapeDtypeStruct((count, 2, V_DIM), jnp.float32)
    )(arrived)
    return lax.all_to_all(prefix, ZY, 0, 0, tiled=True).reshape(RETAIN_KEY_SIZE, V_DIM)


def weight_of_head(ret_key, ret_value):
    rows = ret_key.shape[0]
    heads = lax.axis_size(CORE)
    keys = ret_key.reshape(rows, heads, RETAIN_KEY_SIZE)
    values = ret_value.reshape(rows, heads, V_DIM)
    both = jnp.moveaxis(jnp.concatenate([keys, values], axis=2), 1, 0)
    core = lax.axis_index(CORE)
    mine = lax.dynamic_index_in_dim(both, core, 0, keepdims=False)
    theirs = lax.dynamic_index_in_dim(both, 1 - core, 0, keepdims=False)
    block = in_core_order(mine, core_swap(theirs), 0)
    arrived = from_everyone(block, ZY)
    return arrived.reshape(-1, block.shape[-1])


def gathered_rows(value, axis):
    size = lax.axis_size(axis)
    pieces = [value] + [
        lax.ppermute(value, axis, [((k + step) % size, k) for k in range(size)])
        for step in range(1, size)
    ]
    turned = jnp.concatenate(pieces + pieces[:-1], axis=0)
    start = (size - lax.axis_index(axis)) % size * value.shape[0]
    return lax.dynamic_slice_in_dim(turned, start, size * value.shape[0], 0)


def chain_of_head(kv, log_decay, anchor):
    length = kv.shape[0]
    blocks = length // BLOCK
    positions = anchor + jnp.arange(length, dtype=jnp.int32)
    keys = (
        rotate(kv[:, None, :RETAIN_KEY_SIZE], positions)[:, 0] * RETAIN_KEY_SIZE ** (-0.5)
    ).astype(jnp.bfloat16)
    values = kv[:, RETAIN_KEY_SIZE:]
    running = jnp.cumsum(log_decay.reshape(blocks, BLOCK), axis=-1)
    closing = running[:, -1]
    faded = (
        keys.reshape(blocks, BLOCK, -1).astype(jnp.float32)
        * jnp.exp(closing[:, None] - running)[..., None]
    ).astype(jnp.bfloat16)
    contrib = jnp.einsum(
        "njd,njv->ndv", faded, values.reshape(blocks, BLOCK, -1), preferred_element_type=jnp.float32
    )
    total = contrib[0]
    for n in range(1, blocks):
        total = total * jnp.exp(closing[n]) + contrib[n]
    state = state_before(total, jnp.sum(closing))
    before = []
    for n in range(blocks):
        before.append(state)
        state = state * jnp.exp(closing[n]) + contrib[n]
    return keys, values, jnp.stack(before)


def retention_path(query_ret, key_ret, value_ret, log_decay, before):
    tok_count, heads_here = (query_ret.shape[0], query_ret.shape[1])
    blocks = tok_count // BLOCK
    q_blocks = query_ret.reshape(blocks, BLOCK, heads_here, RETAIN_KEY_SIZE)
    k_blocks = key_ret.reshape(heads_here, blocks, BLOCK, RETAIN_KEY_SIZE)
    v_blocks = value_ret.reshape(heads_here, blocks, BLOCK, V_DIM)
    running = jnp.cumsum(log_decay.reshape(heads_here, blocks, BLOCK), axis=-1)
    within = running[:, :, :, None] - running[:, :, None, :]
    causal_mask = jnp.arange(BLOCK)[:, None] >= jnp.arange(BLOCK)[None, :]
    weighting = jnp.where(causal_mask, jnp.exp(jnp.minimum(within, 0.0)), 0.0)
    scores = (
        jnp.einsum("nihd,hnjd->hnij", q_blocks, k_blocks, preferred_element_type=jnp.float32)
        * weighting
    )
    in_block = jnp.einsum(
        "hnij,hnjv->nihv", scores.astype(jnp.bfloat16), v_blocks, preferred_element_type=jnp.float32
    )
    query_fade = (
        q_blocks.astype(jnp.float32) * jnp.exp(running).transpose(1, 2, 0)[..., None]
    ).astype(jnp.bfloat16)
    carried_term = jnp.einsum("nihd,hndv->nihv", query_fade.astype(jnp.float32), before)
    final_product = in_block + carried_term
    final_product = final_product * lax.rsqrt(
        jnp.mean(final_product * final_product, axis=-1, keepdims=True) + epsilon
    )
    return final_product.reshape(tok_count, heads_here * V_DIM).astype(jnp.bfloat16)


def attention_path(query_att, stacked, sink_logits, anchor):
    tok_count = query_att.shape[0]
    kv_here = stacked.shape[1] // (2 * HEAD_DIM)
    group_size = query_att.shape[1] // (kv_here * HEAD_DIM)
    blocks = tok_count // WINDOW
    extended = stacked.reshape(blocks + 1, WINDOW, 2, kv_here, HEAD_DIM)
    paired = jnp.concatenate([extended[:-1], extended[1:]], axis=1)
    keys_pair = paired[:, :, 0]
    values_pair = paired[:, :, 1]
    q_blocks = query_att.reshape(blocks, WINDOW, kv_here, group_size, HEAD_DIM)
    scores = jnp.einsum(
        "nihgd,njhd->nhgij", q_blocks, keys_pair, preferred_element_type=jnp.float32
    ) * HEAD_DIM ** (-0.5)
    query_pos = anchor + (jnp.arange(blocks) * WINDOW)[:, None] + jnp.arange(WINDOW)[None, :]
    key_pos = (
        anchor + (jnp.arange(blocks) * WINDOW - WINDOW)[:, None] + jnp.arange(2 * WINDOW)[None, :]
    )
    allowed = (
        (key_pos[:, None, :] >= 0)
        & (key_pos[:, None, :] <= query_pos[:, :, None])
        & (query_pos[:, :, None] - key_pos[:, None, :] < WINDOW)
    )
    scores = jnp.where(allowed[:, None, None], scores, masked_out)
    sink_logit = sink_logits.reshape(kv_here, group_size)[None, :, :, None]
    highest = jnp.maximum(jnp.max(scores, axis=-1), sink_logit)
    lifted = jnp.exp(scores - highest[..., None])
    denominator = jnp.sum(lifted, axis=-1) + jnp.exp(sink_logit - highest)
    attn_weights = (lifted / denominator[..., None]).astype(jnp.bfloat16)
    final_product = jnp.einsum(
        "nhgij,njhd->nihgd", attn_weights, values_pair, preferred_element_type=jnp.float32
    )
    return final_product.reshape(tok_count, kv_here * group_size * HEAD_DIM).astype(jnp.bfloat16)


def on_device(
    tokens,
    norm_gain,
    ret_query,
    ret_key,
    ret_value,
    log_decay,
    att_query,
    att_key,
    att_value,
    sink_logits,
    ret_out,
    att_out,
):
    core = lax.axis_index(CORE)
    tok_float = tokens.astype(jnp.float32)
    normed = (
        tok_float
        * lax.rsqrt(jnp.mean(tok_float * tok_float, axis=-1, keepdims=True) + epsilon)
        * norm_gain
    ).astype(jnp.bfloat16)
    weights = (ret_query, att_query, att_key, att_value)
    widths = [weight.shape[1] for weight in weights]
    points = [sum(widths[:index]) for index in range(1, len(widths))]
    whole = lax.all_gather(
        jnp.concatenate([*weights, ret_out.T, att_out.T], axis=1), SP, axis=0, tiled=True
    )
    head_weight = weight_of_head(ret_key, ret_value)
    own_rows = gathered_rows(normed, "tp")
    other_rows = core_swap(own_rows)
    tok_count = own_rows.shape[0]
    rim = shifted(own_rows[tok_count - WINDOW :], SP, 1)
    chip_rows = jnp.concatenate([own_rows, other_rows], axis=0)
    kv = jnp.dot(chip_rows, head_weight, preferred_element_type=jnp.float32).astype(jnp.bfloat16)
    kv = kv.reshape(2, tok_count, kv.shape[-1])
    decay_other = core_swap(log_decay)
    own_head = lax.dynamic_index_in_dim(log_decay, core, 0, keepdims=False)
    other_half = lax.dynamic_index_in_dim(decay_other, core, 0, keepdims=False)
    anchor = lax.axis_index(SP) * tok_count
    chip_anchor = lax.axis_index(ZY) * (2 * tok_count)
    keys, values, before = chain_of_head(
        in_core_order(kv[0], kv[1], 0), in_core_order(own_head, other_half, 0), chip_anchor
    )

    def heads_of_own_rows(value):
        halves = value.reshape(2, value.shape[0] // 2, *value.shape[1:])
        mine = lax.dynamic_index_in_dim(halves, core, 0, keepdims=False)
        theirs = lax.dynamic_index_in_dim(halves, 1 - core, 0, keepdims=False)
        return in_core_order(mine[None], core_swap(theirs)[None], 0)

    key_ret = heads_of_own_rows(keys)
    value_ret = heads_of_own_rows(values)
    before = heads_of_own_rows(before)

    input_width = sum(widths)
    projected = jnp.dot(
        own_rows, whole[:, :input_width], preferred_element_type=jnp.float32
    ).astype(jnp.bfloat16)
    rim_kv = jnp.dot(
        rim, whole[:, points[1] : input_width], preferred_element_type=jnp.float32
    ).astype(jnp.bfloat16)
    sections = jnp.split(projected, points, axis=1)
    stacked = jnp.concatenate([rim_kv, projected[:, points[1] :]], axis=0)
    positions = anchor + jnp.arange(tok_count, dtype=jnp.int32)
    query_ret = rotate(sections[0].reshape(tok_count, -1, RETAIN_KEY_SIZE), positions).astype(
        jnp.bfloat16
    )
    ret_mix = retention_path(query_ret, key_ret, value_ret, log_decay, before)
    att_mix = attention_path(sections[1], stacked, sink_logits, anchor)
    mixes = jnp.concatenate([ret_mix, att_mix], axis=1)
    partial = lax.dot_general(
        mixes,
        whole[:, input_width:],
        (((1,), (1,)), ((), ())),
        preferred_element_type=jnp.float32,
    )
    mixed = sent_and_summed(partial.astype(jnp.bfloat16), "tp", 0)
    return mixed.astype(jnp.bfloat16)


def solution(mesh):
    split = Mesh(mesh.devices.reshape(8, 8, 2, mesh.shape["tp"]), ("sp_0", "sp_1", "sp_2", "tp"))
    placed = (
        P(SP_TP, None),
        P(),
        P(SP, "tp"),
        P(SP, "tp"),
        P(SP, "tp"),
        P("tp", SP),
        P(SP, "tp"),
        P(SP, "tp"),
        P(SP, "tp"),
        P("tp"),
        P("tp", SP),
        P("tp", SP),
    )
    return jax.shard_map(
        on_device, mesh=split, in_specs=placed, out_specs=P(SP_TP, None), check_vma=False
    )
```

```python
import jax
import jax.numpy as jnp
from jax import lax
from jax.experimental import pallas as pl
from jax.sharding import Mesh
from jax.sharding import PartitionSpec as P

RETAIN_KEY_SIZE = 128
V_DIM = 256
HEAD_DIM = 64
WINDOW = 128
BLOCK = 128
SP = ("sp_0", "sp_1", "sp_2")
SP_TP = ("sp_0", "sp_1", "sp_2", "tp")


epsilon = 1e-05
rope_base = 10000.0
masked_out = -1e30


def shifted(value, axis, steps):
    count = lax.axis_size(axis)
    initial, last = (max(0, -steps), min(count, count - steps))
    return lax.ppermute(value, axis, [(source, source + steps) for source in range(initial, last)])


def from_everyone(value, axis):
    size = lax.axis_size(axis)
    return lax.all_to_all(
        jnp.broadcast_to(value[None], (size, *value.shape)), axis, 0, 0, tiled=True
    )


def cut_along(value, dim, size):
    before, after = (value.shape[:dim], value.shape[dim + 1 :])
    return jnp.moveaxis(value.reshape(*before, size, -1, *after), dim, 0)


def sent_and_summed(value, axis, dim):
    tiles = cut_along(value, dim, lax.axis_size(axis))
    arrived = lax.all_to_all(tiles, axis, split_axis=0, concat_axis=0, tiled=True)
    return arrived.astype(jnp.float32).sum(axis=0)


def rotate(values, positions):
    half_dim = values.shape[-1] // 2
    inverse = rope_base ** (-jnp.arange(half_dim, dtype=jnp.float32) / half_dim)
    angles = positions.astype(jnp.float32)[:, None] * inverse[None, :]
    cosine = jnp.cos(angles)[:, None, :]
    sine_part = jnp.sin(angles)[:, None, :]
    first_half = values[..., :half_dim].astype(jnp.float32)
    second_half = values[..., half_dim:].astype(jnp.float32)
    return jnp.concatenate(
        [
            first_half * cosine - second_half * sine_part,
            second_half * cosine + first_half * sine_part,
        ],
        axis=-1,
    )


ZY = ("sp_0", "sp_1")
CORE = "sp_2"


def core_swap(value):
    return lax.ppermute(value, CORE, [(0, 1), (1, 0)])


def in_core_order(own, other, axis):
    first = lax.axis_index(CORE) == 0
    return jnp.concatenate(
        [jnp.where(first, own, other), jnp.where(first, other, own)], axis=axis
    )


def prefix_body(parts_ref, out_ref):
    count = parts_ref.shape[0]
    carried = jnp.zeros(out_ref.shape[1:], jnp.float32)
    for k in range(count):
        out_ref[k] = carried
        carried = carried * jnp.exp(parts_ref[k, 2:3]) + parts_ref[k, :2]


def state_before(total, log_total):
    count = lax.axis_size(ZY)
    slices = total.reshape(count, 2, V_DIM)
    marks = jnp.broadcast_to(log_total, (count, 1, V_DIM))
    sent = jnp.concatenate([slices, marks], axis=1)
    arrived = lax.all_to_all(sent, ZY, 0, 0, tiled=True)
    prefix = pl.pallas_call(
        prefix_body, out_shape=jax.ShapeDtypeStruct((count, 2, V_DIM), jnp.float32)
    )(arrived)
    return lax.all_to_all(prefix, ZY, 0, 0, tiled=True).reshape(RETAIN_KEY_SIZE, V_DIM)


def columns_of_head(ret_key, ret_value, head):
    return jnp.concatenate(
        [
            lax.dynamic_slice_in_dim(ret_key, head * RETAIN_KEY_SIZE, RETAIN_KEY_SIZE, 1),
            lax.dynamic_slice_in_dim(ret_value, head * V_DIM, V_DIM, 1),
        ],
        axis=1,
    )


def weight_of_head(ret_key, ret_value):
    core = lax.axis_index(CORE)
    mine = columns_of_head(ret_key, ret_value, core)
    theirs = core_swap(columns_of_head(ret_key, ret_value, 1 - core))
    block = in_core_order(mine, theirs, 0)
    arrived = from_everyone(block, ZY)
    return arrived.reshape(-1, block.shape[-1])


def gathered_rows(value, axis):
    size = lax.axis_size(axis)
    pieces = [value] + [
        lax.ppermute(value, axis, [((k + step) % size, k) for k in range(size)])
        for step in range(1, size)
    ]
    turned = jnp.concatenate(pieces + pieces[:-1], axis=0)
    start = (size - lax.axis_index(axis)) % size * value.shape[0]
    return lax.dynamic_slice_in_dim(turned, start, size * value.shape[0], 0)


def chain_of_head(kv, log_decay, anchor):
    length = kv.shape[0]
    blocks = length // BLOCK
    positions = anchor + jnp.arange(length, dtype=jnp.int32)
    keys = (
        rotate(kv[:, None, :RETAIN_KEY_SIZE], positions)[:, 0] * RETAIN_KEY_SIZE ** (-0.5)
    ).astype(jnp.bfloat16)
    values = kv[:, RETAIN_KEY_SIZE:]
    running = jnp.cumsum(log_decay.reshape(blocks, BLOCK), axis=-1)
    closing = running[:, -1]
    faded = (
        keys.reshape(blocks, BLOCK, -1).astype(jnp.float32)
        * jnp.exp(closing[:, None] - running)[..., None]
    ).astype(jnp.bfloat16)
    contrib = jnp.einsum(
        "njd,njv->ndv", faded, values.reshape(blocks, BLOCK, -1), preferred_element_type=jnp.float32
    )
    total = contrib[0]
    for n in range(1, blocks):
        total = total * jnp.exp(closing[n]) + contrib[n]
    state = state_before(total, jnp.sum(closing))
    before = []
    for n in range(blocks):
        before.append(state)
        state = state * jnp.exp(closing[n]) + contrib[n]
    return keys, values, jnp.stack(before)


def retention_path(query_ret, key_ret, value_ret, log_decay, before):
    tok_count, heads_here = (query_ret.shape[0], query_ret.shape[1])
    blocks = tok_count // BLOCK
    q_blocks = query_ret.reshape(blocks, BLOCK, heads_here, RETAIN_KEY_SIZE)
    k_blocks = key_ret.reshape(heads_here, blocks, BLOCK, RETAIN_KEY_SIZE)
    v_blocks = value_ret.reshape(heads_here, blocks, BLOCK, V_DIM)
    running = jnp.cumsum(log_decay.reshape(heads_here, blocks, BLOCK), axis=-1)
    within = running[:, :, :, None] - running[:, :, None, :]
    causal_mask = jnp.arange(BLOCK)[:, None] >= jnp.arange(BLOCK)[None, :]
    weighting = jnp.where(causal_mask, jnp.exp(jnp.minimum(within, 0.0)), 0.0)
    scores = (
        jnp.einsum("nihd,hnjd->hnij", q_blocks, k_blocks, preferred_element_type=jnp.float32)
        * weighting
    )
    in_block = jnp.einsum(
        "hnij,hnjv->nihv", scores.astype(jnp.bfloat16), v_blocks, preferred_element_type=jnp.float32
    )
    query_fade = (
        q_blocks.astype(jnp.float32) * jnp.exp(running).transpose(1, 2, 0)[..., None]
    ).astype(jnp.bfloat16)
    carried_term = jnp.einsum("nihd,hndv->nihv", query_fade.astype(jnp.float32), before)
    final_product = in_block + carried_term
    final_product = final_product * lax.rsqrt(
        jnp.mean(final_product * final_product, axis=-1, keepdims=True) + epsilon
    )
    return final_product.reshape(tok_count, heads_here * V_DIM).astype(jnp.bfloat16)


def attention_path(query_att, stacked, sink_logits, anchor):
    tok_count = query_att.shape[0]
    kv_here = stacked.shape[1] // (2 * HEAD_DIM)
    group_size = query_att.shape[1] // (kv_here * HEAD_DIM)
    blocks = tok_count // WINDOW
    extended = stacked.reshape(blocks + 1, WINDOW, 2, kv_here, HEAD_DIM)
    paired = jnp.concatenate([extended[:-1], extended[1:]], axis=1)
    keys_pair = paired[:, :, 0]
    values_pair = paired[:, :, 1]
    q_blocks = query_att.reshape(blocks, WINDOW, kv_here, group_size, HEAD_DIM)
    scores = jnp.einsum(
        "nihgd,njhd->nhgij", q_blocks, keys_pair, preferred_element_type=jnp.float32
    ) * HEAD_DIM ** (-0.5)
    query_pos = anchor + (jnp.arange(blocks) * WINDOW)[:, None] + jnp.arange(WINDOW)[None, :]
    key_pos = (
        anchor + (jnp.arange(blocks) * WINDOW - WINDOW)[:, None] + jnp.arange(2 * WINDOW)[None, :]
    )
    allowed = (
        (key_pos[:, None, :] >= 0)
        & (key_pos[:, None, :] <= query_pos[:, :, None])
        & (query_pos[:, :, None] - key_pos[:, None, :] < WINDOW)
    )
    scores = jnp.where(allowed[:, None, None], scores, masked_out)
    sink_logit = sink_logits.reshape(kv_here, group_size)[None, :, :, None]
    highest = jnp.maximum(jnp.max(scores, axis=-1), sink_logit)
    lifted = jnp.exp(scores - highest[..., None])
    denominator = jnp.sum(lifted, axis=-1) + jnp.exp(sink_logit - highest)
    attn_weights = (lifted / denominator[..., None]).astype(jnp.bfloat16)
    final_product = jnp.einsum(
        "nhgij,njhd->nihgd", attn_weights, values_pair, preferred_element_type=jnp.float32
    )
    return final_product.reshape(tok_count, kv_here * group_size * HEAD_DIM).astype(jnp.bfloat16)


def on_device(
    tokens,
    norm_gain,
    ret_query,
    ret_key,
    ret_value,
    log_decay,
    att_query,
    att_key,
    att_value,
    sink_logits,
    ret_out,
    att_out,
):
    core = lax.axis_index(CORE)
    tok_float = tokens.astype(jnp.float32)
    normed = (
        tok_float
        * lax.rsqrt(jnp.mean(tok_float * tok_float, axis=-1, keepdims=True) + epsilon)
        * norm_gain
    ).astype(jnp.bfloat16)
    weights = (ret_query, att_query, att_key, att_value)
    widths = [weight.shape[1] for weight in weights]
    points = [sum(widths[:index]) for index in range(1, len(widths))]
    whole = lax.all_gather(
        jnp.concatenate([*weights, ret_out.T, att_out.T], axis=1), SP, axis=0, tiled=True
    )
    head_weight = weight_of_head(ret_key, ret_value)
    own_rows = gathered_rows(normed, "tp")
    other_rows = core_swap(own_rows)
    tok_count = own_rows.shape[0]
    rim = shifted(own_rows[tok_count - WINDOW :], SP, 1)
    chip_rows = jnp.concatenate([own_rows, other_rows], axis=0)
    kv = jnp.dot(chip_rows, head_weight, preferred_element_type=jnp.float32).astype(jnp.bfloat16)
    kv = kv.reshape(2, tok_count, kv.shape[-1])
    decay_other = core_swap(log_decay)
    own_head = lax.dynamic_index_in_dim(log_decay, core, 0, keepdims=False)
    other_half = lax.dynamic_index_in_dim(decay_other, core, 0, keepdims=False)
    anchor = lax.axis_index(SP) * tok_count
    chip_anchor = lax.axis_index(ZY) * (2 * tok_count)
    keys, values, before = chain_of_head(
        in_core_order(kv[0], kv[1], 0), in_core_order(own_head, other_half, 0), chip_anchor
    )

    def heads_of_own_rows(value):
        halves = value.reshape(2, value.shape[0] // 2, *value.shape[1:])
        mine = lax.dynamic_index_in_dim(halves, core, 0, keepdims=False)
        theirs = lax.dynamic_index_in_dim(halves, 1 - core, 0, keepdims=False)
        return in_core_order(mine[None], core_swap(theirs)[None], 0)

    key_ret = heads_of_own_rows(keys)
    value_ret = heads_of_own_rows(values)
    before = heads_of_own_rows(before)

    input_width = sum(widths)
    projected = jnp.dot(
        own_rows, whole[:, :input_width], preferred_element_type=jnp.float32
    ).astype(jnp.bfloat16)
    rim_kv = jnp.dot(
        rim, whole[:, points[1] : input_width], preferred_element_type=jnp.float32
    ).astype(jnp.bfloat16)
    sections = jnp.split(projected, points, axis=1)
    stacked = jnp.concatenate([rim_kv, projected[:, points[1] :]], axis=0)
    positions = anchor + jnp.arange(tok_count, dtype=jnp.int32)
    query_ret = rotate(sections[0].reshape(tok_count, -1, RETAIN_KEY_SIZE), positions).astype(
        jnp.bfloat16
    )
    ret_mix = retention_path(query_ret, key_ret, value_ret, log_decay, before)
    att_mix = attention_path(sections[1], stacked, sink_logits, anchor)
    mixes = jnp.concatenate([ret_mix, att_mix], axis=1)
    partial = lax.dot_general(
        mixes,
        whole[:, input_width:],
        (((1,), (1,)), ((), ())),
        preferred_element_type=jnp.float32,
    )
    mixed = sent_and_summed(partial.astype(jnp.bfloat16), "tp", 0)
    return mixed.astype(jnp.bfloat16)


def solution(mesh):
    split = Mesh(mesh.devices.reshape(8, 8, 2, mesh.shape["tp"]), ("sp_0", "sp_1", "sp_2", "tp"))
    placed = (
        P(SP_TP, None),
        P(),
        P(SP, "tp"),
        P(SP, "tp"),
        P(SP, "tp"),
        P("tp", SP),
        P(SP, "tp"),
        P(SP, "tp"),
        P(SP, "tp"),
        P("tp"),
        P("tp", SP),
        P("tp", SP),
    )
    return jax.shard_map(
        on_device, mesh=split, in_specs=placed, out_specs=P(SP_TP, None), check_vma=False
    )
```

```python
import jax
import jax.numpy as jnp
from jax import lax
from jax.experimental import pallas as pl
from jax.experimental.pallas import tpu as pltpu
from jax.sharding import Mesh
from jax.sharding import PartitionSpec as P

RETAIN_KEY_SIZE = 128
V_DIM = 256
HEAD_DIM = 64
WINDOW = 128
BLOCK = 128
SP = ("sp_0", "sp_1", "sp_2")
SP_TP = ("sp_0", "sp_1", "sp_2", "tp")


epsilon = 1e-05
rope_base = 10000.0
masked_out = -1e30


def shifted(value, axis, steps):
    count = lax.axis_size(axis)
    initial, last = (max(0, -steps), min(count, count - steps))
    return lax.ppermute(value, axis, [(source, source + steps) for source in range(initial, last)])


def from_everyone(value, axis):
    size = lax.axis_size(axis)
    return lax.all_to_all(
        jnp.broadcast_to(value[None], (size, *value.shape)), axis, 0, 0, tiled=True
    )


def cut_along(value, dim, size):
    before, after = (value.shape[:dim], value.shape[dim + 1 :])
    return jnp.moveaxis(value.reshape(*before, size, -1, *after), dim, 0)


def sent_and_summed(value, axis, dim):
    tiles = cut_along(value, dim, lax.axis_size(axis))
    arrived = lax.all_to_all(tiles, axis, split_axis=0, concat_axis=0, tiled=True)
    return arrived.astype(jnp.float32).sum(axis=0)


def rotate(values, positions):
    half_dim = values.shape[-1] // 2
    inverse = rope_base ** (-jnp.arange(half_dim, dtype=jnp.float32) / half_dim)
    angles = positions.astype(jnp.float32)[:, None] * inverse[None, :]
    cosine = jnp.cos(angles)[:, None, :]
    sine_part = jnp.sin(angles)[:, None, :]
    first_half = values[..., :half_dim].astype(jnp.float32)
    second_half = values[..., half_dim:].astype(jnp.float32)
    return jnp.concatenate(
        [
            first_half * cosine - second_half * sine_part,
            second_half * cosine + first_half * sine_part,
        ],
        axis=-1,
    )


ZY = ("sp_0", "sp_1")
CORE = "sp_2"


def core_swap(value):
    return lax.ppermute(value, CORE, [(0, 1), (1, 0)])


def in_core_order(own, other, axis):
    first = lax.axis_index(CORE) == 0
    return jnp.concatenate(
        [jnp.where(first, own, other), jnp.where(first, other, own)], axis=axis
    )


def prefix_body(parts_ref, out_ref):
    count = parts_ref.shape[0]
    carried = jnp.zeros(out_ref.shape[1:], jnp.float32)
    for k in range(count):
        out_ref[k] = carried
        carried = carried * jnp.exp(parts_ref[k, 2:3]) + parts_ref[k, :2]


def state_before(total, log_total):
    count = lax.axis_size(ZY)
    slices = total.reshape(count, 2, V_DIM)
    marks = jnp.broadcast_to(log_total, (count, 1, V_DIM))
    sent = jnp.concatenate([slices, marks], axis=1)
    arrived = lax.all_to_all(sent, ZY, 0, 0, tiled=True)
    prefix = pl.pallas_call(
        prefix_body, out_shape=jax.ShapeDtypeStruct((count, 2, V_DIM), jnp.float32)
    )(arrived)
    return lax.all_to_all(prefix, ZY, 0, 0, tiled=True).reshape(RETAIN_KEY_SIZE, V_DIM)


def columns_of_head(ret_key, ret_value, head):
    return jnp.concatenate(
        [
            lax.dynamic_slice_in_dim(ret_key, head * RETAIN_KEY_SIZE, RETAIN_KEY_SIZE, 1),
            lax.dynamic_slice_in_dim(ret_value, head * V_DIM, V_DIM, 1),
        ],
        axis=1,
    )


def weight_of_head(ret_key, ret_value):
    core = lax.axis_index(CORE)
    mine = columns_of_head(ret_key, ret_value, core)
    theirs = core_swap(columns_of_head(ret_key, ret_value, 1 - core))
    block = in_core_order(mine, theirs, 0)
    arrived = from_everyone(block, ZY)
    return arrived.reshape(-1, block.shape[-1])


def gathered_rows(value, axis):
    size = lax.axis_size(axis)
    pieces = [value] + [
        lax.ppermute(value, axis, [((k + step) % size, k) for k in range(size)])
        for step in range(1, size)
    ]
    turned = jnp.concatenate(pieces + pieces[:-1], axis=0)
    start = (size - lax.axis_index(axis)) % size * value.shape[0]
    return lax.dynamic_slice_in_dim(turned, start, size * value.shape[0], 0)


def chain_of_head(kv, log_decay, anchor):
    length = kv.shape[0]
    blocks = length // BLOCK
    positions = anchor + jnp.arange(length, dtype=jnp.int32)
    keys = (
        rotate(kv[:, None, :RETAIN_KEY_SIZE], positions)[:, 0] * RETAIN_KEY_SIZE ** (-0.5)
    ).astype(jnp.bfloat16)
    values = kv[:, RETAIN_KEY_SIZE:]
    running = jnp.cumsum(log_decay.reshape(blocks, BLOCK), axis=-1)
    closing = running[:, -1]
    faded = (
        keys.reshape(blocks, BLOCK, -1).astype(jnp.float32)
        * jnp.exp(closing[:, None] - running)[..., None]
    ).astype(jnp.bfloat16)
    contrib = jnp.einsum(
        "njd,njv->ndv", faded, values.reshape(blocks, BLOCK, -1), preferred_element_type=jnp.float32
    )
    total = contrib[0]
    for n in range(1, blocks):
        total = total * jnp.exp(closing[n]) + contrib[n]
    state = state_before(total, jnp.sum(closing))
    before = []
    for n in range(blocks):
        before.append(state)
        state = state * jnp.exp(closing[n]) + contrib[n]
    return keys, values, jnp.stack(before)


CHUNKS = 4


def tail_body(
    rows_ref, key_ref, value_ref, before_ref, weight_ref, fade_ref, cos_ref, sin_ref, bias_ref,
    sink_ref, whole_ref, out_ref, win_ref, wout_ref, ret_ref, att_ref, sems,
):
    width, in_width = (rows_ref.shape[1], win_ref.shape[1])
    length = out_ref.shape[0]
    step = width // CHUNKS
    copies = [
        pltpu.make_async_copy(
            whole_ref.at[pl.ds(k * step, step), pl.ds(0, in_width)],
            win_ref.at[pl.ds(k * step, step)],
            sems.at[k],
        )
        for k in range(CHUNKS)
    ]
    copies.append(
        pltpu.make_async_copy(
            whole_ref.at[:, pl.ds(in_width, wout_ref.shape[1])], wout_ref, sems.at[CHUNKS]
        )
    )
    for copy in copies:
        copy.start()
    total = None
    for k in range(CHUNKS):
        copies[k].wait()
        part = jnp.dot(
            rows_ref[:, k * step : (k + 1) * step],
            win_ref[k * step : (k + 1) * step],
            preferred_element_type=jnp.float32,
        )
        total = part if total is None else total + part
    projected = total.astype(jnp.bfloat16)
    heads, blocks = (before_ref.shape[0], before_ref.shape[1])
    rim = rows_ref.shape[0] - length
    cosine = cos_ref[...]
    sine_part = sin_ref[...]
    contract_last = (((1,), (1,)), ((), ()))
    for h in range(heads):
        query = projected[rim:, h * RETAIN_KEY_SIZE : (h + 1) * RETAIN_KEY_SIZE].astype(jnp.float32)
        turned = pltpu.roll(query, RETAIN_KEY_SIZE // 2, 1)
        query = (query * cosine + turned * sine_part).astype(jnp.bfloat16)
        faded = (query.astype(jnp.float32) * fade_ref[h]).astype(jnp.bfloat16)
        for n in range(blocks):
            part = slice(n * BLOCK, (n + 1) * BLOCK)
            scores = lax.dot_general(
                query[part], key_ref[h, part], contract_last, preferred_element_type=jnp.float32
            )
            scores = (scores * weight_ref[h, n]).astype(jnp.bfloat16)
            mixed = jnp.dot(scores, value_ref[h, part], preferred_element_type=jnp.float32)
            mixed = mixed + jnp.dot(faded[part], before_ref[h, n], preferred_element_type=jnp.float32)
            mixed = mixed * lax.rsqrt(jnp.mean(mixed * mixed, axis=-1, keepdims=True) + epsilon)
            ret_ref[part, h * V_DIM : (h + 1) * V_DIM] = mixed.astype(jnp.bfloat16)
    first = heads * RETAIN_KEY_SIZE
    group = sink_ref.shape[0]
    keys_at = first + group * HEAD_DIM
    keys = projected[:, keys_at : keys_at + HEAD_DIM]
    values = projected[:, keys_at + HEAD_DIM : keys_at + 2 * HEAD_DIM]
    for n in range(length // WINDOW):
        seen = slice(n * WINDOW, (n + 2) * WINDOW)
        bias = bias_ref[n]
        for g in range(0, group, 2):
            pair = []
            for k in (g, g + 1):
                at = first + k * HEAD_DIM
                query = projected[rim + n * WINDOW : rim + (n + 1) * WINDOW, at : at + HEAD_DIM]
                scores = lax.dot_general(
                    query, keys[seen], contract_last, preferred_element_type=jnp.float32
                )
                scores = scores * HEAD_DIM ** (-0.5) + bias
                sink = jnp.full((WINDOW, 1), sink_ref[k], jnp.float32)
                highest = jnp.maximum(jnp.max(scores, axis=-1, keepdims=True), sink)
                lifted = jnp.exp(scores - highest)
                below = jnp.sum(lifted, axis=-1, keepdims=True) + jnp.exp(sink - highest)
                found = jnp.dot(
                    lifted.astype(jnp.bfloat16), values[seen], preferred_element_type=jnp.float32
                )
                pair.append(found / below)
            att_ref[n * WINDOW : (n + 1) * WINDOW, g * HEAD_DIM : (g + 2) * HEAD_DIM] = (
                jnp.concatenate(pair, axis=1).astype(jnp.bfloat16)
            )
    copies[CHUNKS].wait()
    half = ret_ref.shape[1]
    result = lax.dot_general(
        ret_ref[...], wout_ref[:, :half], contract_last, preferred_element_type=jnp.float32
    ) + lax.dot_general(
        att_ref[...], wout_ref[:, half:], contract_last, preferred_element_type=jnp.float32
    )
    out_ref[...] = result.astype(jnp.bfloat16)


def tail(rows, keys, values, before, log_decay, sink_logits, whole, anchor, in_width):
    length = keys.shape[1]
    heads, blocks = (before.shape[0], before.shape[1])
    running = jnp.cumsum(log_decay.reshape(heads, blocks, BLOCK), axis=-1)
    within = running[:, :, :, None] - running[:, :, None, :]
    causal_mask = jnp.arange(BLOCK)[:, None] >= jnp.arange(BLOCK)[None, :]
    weighting = jnp.where(causal_mask, jnp.exp(jnp.minimum(within, 0.0)), 0.0)
    fade = jnp.exp(running).reshape(heads, length, 1)
    half_dim = RETAIN_KEY_SIZE // 2
    inverse = rope_base ** (-jnp.arange(half_dim, dtype=jnp.float32) / half_dim)
    positions = anchor + jnp.arange(length, dtype=jnp.int32)
    angles = positions.astype(jnp.float32)[:, None] * inverse[None, :]
    cosine = jnp.concatenate([jnp.cos(angles)] * 2, axis=1)
    sine_part = jnp.concatenate([-jnp.sin(angles), jnp.sin(angles)], axis=1)
    starts = jnp.arange(length // WINDOW)[:, None, None] * WINDOW
    ahead = jnp.arange(2 * WINDOW)[None, None, :] - jnp.arange(WINDOW)[None, :, None]
    there = anchor + starts - WINDOW + jnp.arange(2 * WINDOW)[None, None, :] >= 0
    bias = jnp.where((ahead > 0) & (ahead <= WINDOW) & there, 0.0, masked_out)
    out_width = whole.shape[1] - in_width
    features = rows.shape[1]
    columns = whole.shape[0]
    vmem = pl.BlockSpec(memory_space=pltpu.VMEM)
    return pl.pallas_call(
        tail_body,
        out_shape=jax.ShapeDtypeStruct((length, columns), jnp.bfloat16),
        in_specs=[vmem] * 9
        + [pl.BlockSpec(memory_space=pltpu.SMEM), pl.BlockSpec(memory_space=pltpu.HBM)],
        out_specs=vmem,
        scratch_shapes=[
            pltpu.VMEM((features, in_width), jnp.bfloat16),
            pltpu.VMEM((columns, out_width), jnp.bfloat16),
            pltpu.VMEM((length, heads * V_DIM), jnp.bfloat16),
            pltpu.VMEM((length, sink_logits.shape[0] * HEAD_DIM), jnp.bfloat16),
            pltpu.SemaphoreType.DMA((CHUNKS + 1,)),
        ],
        compiler_params=pltpu.CompilerParams(vmem_limit_bytes=40 * 1024 * 1024),
        name="tail",
    )(rows, keys, values, before, weighting, fade, cosine, sine_part, bias, sink_logits,
      pltpu.with_memory_space_constraint(whole, pltpu.HBM))


def on_device(
    tokens,
    norm_gain,
    ret_query,
    ret_key,
    ret_value,
    log_decay,
    att_query,
    att_key,
    att_value,
    sink_logits,
    ret_out,
    att_out,
):
    core = lax.axis_index(CORE)
    tok_float = tokens.astype(jnp.float32)
    normed = (
        tok_float
        * lax.rsqrt(jnp.mean(tok_float * tok_float, axis=-1, keepdims=True) + epsilon)
        * norm_gain
    ).astype(jnp.bfloat16)
    weights = (ret_query, att_query, att_key, att_value)
    widths = [weight.shape[1] for weight in weights]
    whole = lax.all_gather(
        jnp.concatenate([*weights, ret_out.T, att_out.T], axis=1), SP, axis=0, tiled=True
    )
    head_weight = weight_of_head(ret_key, ret_value)
    own_rows = gathered_rows(normed, "tp")
    other_rows = core_swap(own_rows)
    tok_count = own_rows.shape[0]
    rim = shifted(own_rows[tok_count - WINDOW :], SP, 1)
    chip_rows = jnp.concatenate([own_rows, other_rows], axis=0)
    kv = jnp.dot(chip_rows, head_weight, preferred_element_type=jnp.float32).astype(jnp.bfloat16)
    kv = kv.reshape(2, tok_count, kv.shape[-1])
    decay_other = core_swap(log_decay)
    own_head = lax.dynamic_index_in_dim(log_decay, core, 0, keepdims=False)
    other_half = lax.dynamic_index_in_dim(decay_other, core, 0, keepdims=False)
    anchor = lax.axis_index(SP) * tok_count
    chip_anchor = lax.axis_index(ZY) * (2 * tok_count)
    keys, values, before = chain_of_head(
        in_core_order(kv[0], kv[1], 0), in_core_order(own_head, other_half, 0), chip_anchor
    )

    def heads_of_own_rows(value):
        halves = value.reshape(2, value.shape[0] // 2, *value.shape[1:])
        mine = lax.dynamic_index_in_dim(halves, core, 0, keepdims=False)
        theirs = lax.dynamic_index_in_dim(halves, 1 - core, 0, keepdims=False)
        return in_core_order(mine[None], core_swap(theirs)[None], 0)

    key_ret = heads_of_own_rows(keys)
    value_ret = heads_of_own_rows(values)
    before = heads_of_own_rows(before)

    input_width = sum(widths)
    partial = tail(
        jnp.concatenate([rim, own_rows], axis=0),
        key_ret,
        value_ret,
        before.astype(jnp.bfloat16),
        log_decay,
        sink_logits,
        whole,
        anchor,
        input_width,
    )
    mixed = sent_and_summed(partial, "tp", 0)
    return mixed.astype(jnp.bfloat16)


def solution(mesh):
    split = Mesh(mesh.devices.reshape(8, 8, 2, mesh.shape["tp"]), ("sp_0", "sp_1", "sp_2", "tp"))
    placed = (
        P(SP_TP, None),
        P(),
        P(SP, "tp"),
        P(SP, "tp"),
        P(SP, "tp"),
        P("tp", SP),
        P(SP, "tp"),
        P(SP, "tp"),
        P(SP, "tp"),
        P("tp"),
        P("tp", SP),
        P("tp", SP),
    )
    return jax.shard_map(
        on_device, mesh=split, in_specs=placed, out_specs=P(SP_TP, None), check_vma=False
    )
```

```python
import jax
import jax.numpy as jnp
from jax import lax
from jax.experimental import pallas as pl
from jax.experimental.pallas import tpu as pltpu
from jax.sharding import Mesh
from jax.sharding import PartitionSpec as P

RETAIN_KEY_SIZE = 128
V_DIM = 256
HEAD_DIM = 64
WINDOW = 128
BLOCK = 128
SP = ("sp_0", "sp_1", "sp_2")
SP_TP = ("sp_0", "sp_1", "sp_2", "tp")


epsilon = 1e-05
rope_base = 10000.0
masked_out = -1e30


def shifted(value, axis, steps):
    count = lax.axis_size(axis)
    initial, last = (max(0, -steps), min(count, count - steps))
    return lax.ppermute(value, axis, [(source, source + steps) for source in range(initial, last)])


def from_everyone(value, axis):
    size = lax.axis_size(axis)
    return lax.all_to_all(
        jnp.broadcast_to(value[None], (size, *value.shape)), axis, 0, 0, tiled=True
    )


def moved(value, axis, step):
    size = lax.axis_size(axis)
    return lax.ppermute(value, axis, [(k, (k + step) % size) for k in range(size)])


def added(first, second):
    return (first.astype(jnp.float32) + second.astype(jnp.float32)).astype(jnp.bfloat16)


def summed_over_four(value, axis):
    size = lax.axis_size(axis)
    here = lax.axis_index(axis)
    tiles = value.reshape(size, -1, value.shape[-1])
    half = tiles.shape[1] // 2

    def for_device(step):
        return lax.dynamic_index_in_dim(tiles, (here + step) % size, 0, keepdims=False)

    far = for_device(2)
    from_below = moved(far[half:], axis, 1)
    from_above = moved(far[:half], axis, -1)
    up = for_device(1)
    down = for_device(3)
    up = jnp.concatenate([up[:half], added(up[half:], from_below)], axis=0)
    down = jnp.concatenate([added(down[:half], from_above), down[half:]], axis=0)
    return (
        for_device(0).astype(jnp.float32)
        + moved(up, axis, 1).astype(jnp.float32)
        + moved(down, axis, -1).astype(jnp.float32)
    )


def rotate(values, positions):
    half_dim = values.shape[-1] // 2
    inverse = rope_base ** (-jnp.arange(half_dim, dtype=jnp.float32) / half_dim)
    angles = positions.astype(jnp.float32)[:, None] * inverse[None, :]
    cosine = jnp.cos(angles)[:, None, :]
    sine_part = jnp.sin(angles)[:, None, :]
    first_half = values[..., :half_dim].astype(jnp.float32)
    second_half = values[..., half_dim:].astype(jnp.float32)
    return jnp.concatenate(
        [
            first_half * cosine - second_half * sine_part,
            second_half * cosine + first_half * sine_part,
        ],
        axis=-1,
    )


ZY = ("sp_0", "sp_1")
CORE = "sp_2"


def core_swap(value):
    return lax.ppermute(value, CORE, [(0, 1), (1, 0)])


def in_core_order(own, other, axis):
    first = lax.axis_index(CORE) == 0
    return jnp.concatenate(
        [jnp.where(first, own, other), jnp.where(first, other, own)], axis=axis
    )


def prefix_body(parts_ref, out_ref):
    count = parts_ref.shape[0]
    carried = jnp.zeros(out_ref.shape[1:], jnp.float32)
    for k in range(count):
        out_ref[k] = carried
        carried = carried * jnp.exp(parts_ref[k, 2:3]) + parts_ref[k, :2]


def state_before(total, log_total):
    count = lax.axis_size(ZY)
    slices = total.reshape(count, 2, V_DIM)
    marks = jnp.broadcast_to(log_total, (count, 1, V_DIM))
    sent = jnp.concatenate([slices, marks], axis=1)
    arrived = lax.all_to_all(sent, ZY, 0, 0, tiled=True)
    prefix = pl.pallas_call(
        prefix_body, out_shape=jax.ShapeDtypeStruct((count, 2, V_DIM), jnp.float32)
    )(arrived)
    return lax.all_to_all(prefix, ZY, 0, 0, tiled=True).reshape(RETAIN_KEY_SIZE, V_DIM)


def columns_of_head(ret_key, ret_value, head):
    return jnp.concatenate(
        [
            lax.dynamic_slice_in_dim(ret_key, head * RETAIN_KEY_SIZE, RETAIN_KEY_SIZE, 1),
            lax.dynamic_slice_in_dim(ret_value, head * V_DIM, V_DIM, 1),
        ],
        axis=1,
    )


def weight_of_head(ret_key, ret_value):
    core = lax.axis_index(CORE)
    mine = columns_of_head(ret_key, ret_value, core)
    theirs = core_swap(columns_of_head(ret_key, ret_value, 1 - core))
    block = in_core_order(mine, theirs, 0)
    arrived = from_everyone(block, "sp_1")
    part = arrived.reshape(-1, block.shape[-1])
    return ring_gathered(part, "sp_0")


def ring_gathered(part, axis):
    size = lax.axis_size(axis)
    here = lax.axis_index(axis)
    rows = part.shape[0]
    whole = jnp.zeros((size * rows, part.shape[1]), part.dtype)

    def put(whole, value, owner, offset=0):
        return lax.dynamic_update_slice_in_dim(whole, value, owner % size * rows + offset, 0)

    whole = put(whole, part, here)
    up = down = part
    for step in range(1, size // 2):
        up = moved(up, axis, 1)
        down = moved(down, axis, -1)
        whole = put(whole, up, here - step + size)
        whole = put(whole, down, here + step)
    half = rows // 2
    up = moved(up[:half], axis, 1)
    down = moved(down[half:], axis, -1)
    whole = put(whole, up, here + size // 2)
    return put(whole, down, here + size // 2, half)


def gathered_rows(value, axis):
    size = lax.axis_size(axis)
    here = lax.axis_index(axis)
    rows = value.shape[0]
    whole = jnp.zeros((size * rows, value.shape[1]), value.dtype)
    whole = lax.dynamic_update_slice_in_dim(whole, value, here * rows, 0)
    for step in range(1, size):
        piece = moved(value, axis, step)
        whole = lax.dynamic_update_slice_in_dim(
            whole, piece, (here - step + size) % size * rows, 0
        )
    return whole


def chain_of_head(kv, log_decay, anchor):
    length = kv.shape[0]
    blocks = length // BLOCK
    positions = anchor + jnp.arange(length, dtype=jnp.int32)
    keys = (
        rotate(kv[:, None, :RETAIN_KEY_SIZE], positions)[:, 0] * RETAIN_KEY_SIZE ** (-0.5)
    ).astype(jnp.bfloat16)
    values = kv[:, RETAIN_KEY_SIZE:]
    running = jnp.cumsum(log_decay.reshape(blocks, BLOCK), axis=-1)
    closing = running[:, -1]
    faded = (
        keys.reshape(blocks, BLOCK, -1).astype(jnp.float32)
        * jnp.exp(closing[:, None] - running)[..., None]
    ).astype(jnp.bfloat16)
    contrib = jnp.einsum(
        "njd,njv->ndv", faded, values.reshape(blocks, BLOCK, -1), preferred_element_type=jnp.float32
    )
    total = contrib[0]
    for n in range(1, blocks):
        total = total * jnp.exp(closing[n]) + contrib[n]
    state = state_before(total, jnp.sum(closing))
    before = []
    for n in range(blocks):
        before.append(state)
        state = state * jnp.exp(closing[n]) + contrib[n]
    return keys, values, jnp.stack(before)


CHUNKS = 4


def tail_body(
    rows_ref, key_ref, value_ref, before_ref, weight_ref, fade_ref, cos_ref, sin_ref, bias_ref,
    sink_ref, whole_ref, out_ref, win_ref, wout_ref, ret_ref, att_ref, sems,
):
    width, in_width = (rows_ref.shape[1], win_ref.shape[1])
    length = out_ref.shape[0]
    step = width // CHUNKS
    copies = [
        pltpu.make_async_copy(
            whole_ref.at[pl.ds(k * step, step), pl.ds(0, in_width)],
            win_ref.at[pl.ds(k * step, step)],
            sems.at[k],
        )
        for k in range(CHUNKS)
    ]
    copies.append(
        pltpu.make_async_copy(
            whole_ref.at[:, pl.ds(in_width, wout_ref.shape[1])], wout_ref, sems.at[CHUNKS]
        )
    )
    for copy in copies:
        copy.start()
    total = None
    for k in range(CHUNKS):
        copies[k].wait()
        part = jnp.dot(
            rows_ref[:, k * step : (k + 1) * step],
            win_ref[k * step : (k + 1) * step],
            preferred_element_type=jnp.float32,
        )
        total = part if total is None else total + part
    projected = total.astype(jnp.bfloat16)
    heads, blocks = (before_ref.shape[0], before_ref.shape[1])
    rim = rows_ref.shape[0] - length
    cosine = cos_ref[...]
    sine_part = sin_ref[...]
    contract_last = (((1,), (1,)), ((), ()))
    for h in range(heads):
        query = projected[rim:, h * RETAIN_KEY_SIZE : (h + 1) * RETAIN_KEY_SIZE].astype(jnp.float32)
        turned = pltpu.roll(query, RETAIN_KEY_SIZE // 2, 1)
        query = (query * cosine + turned * sine_part).astype(jnp.bfloat16)
        faded = (query.astype(jnp.float32) * fade_ref[h]).astype(jnp.bfloat16)
        for n in range(blocks):
            part = slice(n * BLOCK, (n + 1) * BLOCK)
            scores = lax.dot_general(
                query[part], key_ref[h, part], contract_last, preferred_element_type=jnp.float32
            )
            scores = (scores * weight_ref[h, n]).astype(jnp.bfloat16)
            mixed = jnp.dot(scores, value_ref[h, part], preferred_element_type=jnp.float32)
            mixed = mixed + jnp.dot(faded[part], before_ref[h, n], preferred_element_type=jnp.float32)
            mixed = mixed * lax.rsqrt(jnp.mean(mixed * mixed, axis=-1, keepdims=True) + epsilon)
            ret_ref[part, h * V_DIM : (h + 1) * V_DIM] = mixed.astype(jnp.bfloat16)
    first = heads * RETAIN_KEY_SIZE
    group = sink_ref.shape[0]
    keys_at = first + group * HEAD_DIM
    keys = projected[:, keys_at : keys_at + HEAD_DIM]
    values = projected[:, keys_at + HEAD_DIM : keys_at + 2 * HEAD_DIM]
    for n in range(length // WINDOW):
        seen = slice(n * WINDOW, (n + 2) * WINDOW)
        bias = bias_ref[n]
        for g in range(0, group, 2):
            pair = []
            for k in (g, g + 1):
                at = first + k * HEAD_DIM
                query = projected[rim + n * WINDOW : rim + (n + 1) * WINDOW, at : at + HEAD_DIM]
                scores = lax.dot_general(
                    query, keys[seen], contract_last, preferred_element_type=jnp.float32
                )
                scores = scores * HEAD_DIM ** (-0.5) + bias
                sink = jnp.full((WINDOW, 1), sink_ref[k], jnp.float32)
                highest = jnp.maximum(jnp.max(scores, axis=-1, keepdims=True), sink)
                lifted = jnp.exp(scores - highest)
                below = jnp.sum(lifted, axis=-1, keepdims=True) + jnp.exp(sink - highest)
                found = jnp.dot(
                    lifted.astype(jnp.bfloat16), values[seen], preferred_element_type=jnp.float32
                )
                pair.append(found / below)
            att_ref[n * WINDOW : (n + 1) * WINDOW, g * HEAD_DIM : (g + 2) * HEAD_DIM] = (
                jnp.concatenate(pair, axis=1).astype(jnp.bfloat16)
            )
    copies[CHUNKS].wait()
    half = ret_ref.shape[1]
    result = lax.dot_general(
        ret_ref[...], wout_ref[:, :half], contract_last, preferred_element_type=jnp.float32
    ) + lax.dot_general(
        att_ref[...], wout_ref[:, half:], contract_last, preferred_element_type=jnp.float32
    )
    out_ref[...] = result.astype(jnp.bfloat16)


def tail(rows, keys, values, before, log_decay, sink_logits, whole, anchor, in_width):
    length = keys.shape[1]
    heads, blocks = (before.shape[0], before.shape[1])
    running = jnp.cumsum(log_decay.reshape(heads, blocks, BLOCK), axis=-1)
    within = running[:, :, :, None] - running[:, :, None, :]
    causal_mask = jnp.arange(BLOCK)[:, None] >= jnp.arange(BLOCK)[None, :]
    weighting = jnp.where(causal_mask, jnp.exp(jnp.minimum(within, 0.0)), 0.0)
    fade = jnp.exp(running).reshape(heads, length, 1)
    half_dim = RETAIN_KEY_SIZE // 2
    inverse = rope_base ** (-jnp.arange(half_dim, dtype=jnp.float32) / half_dim)
    positions = anchor + jnp.arange(length, dtype=jnp.int32)
    angles = positions.astype(jnp.float32)[:, None] * inverse[None, :]
    cosine = jnp.concatenate([jnp.cos(angles)] * 2, axis=1)
    sine_part = jnp.concatenate([-jnp.sin(angles), jnp.sin(angles)], axis=1)
    starts = jnp.arange(length // WINDOW)[:, None, None] * WINDOW
    ahead = jnp.arange(2 * WINDOW)[None, None, :] - jnp.arange(WINDOW)[None, :, None]
    there = anchor + starts - WINDOW + jnp.arange(2 * WINDOW)[None, None, :] >= 0
    bias = jnp.where((ahead > 0) & (ahead <= WINDOW) & there, 0.0, masked_out)
    out_width = whole.shape[1] - in_width
    features = rows.shape[1]
    columns = whole.shape[0]
    vmem = pl.BlockSpec(memory_space=pltpu.VMEM)
    return pl.pallas_call(
        tail_body,
        out_shape=jax.ShapeDtypeStruct((length, columns), jnp.bfloat16),
        in_specs=[vmem] * 9
        + [pl.BlockSpec(memory_space=pltpu.SMEM), pl.BlockSpec(memory_space=pltpu.HBM)],
        out_specs=vmem,
        scratch_shapes=[
            pltpu.VMEM((features, in_width), jnp.bfloat16),
            pltpu.VMEM((columns, out_width), jnp.bfloat16),
            pltpu.VMEM((length, heads * V_DIM), jnp.bfloat16),
            pltpu.VMEM((length, sink_logits.shape[0] * HEAD_DIM), jnp.bfloat16),
            pltpu.SemaphoreType.DMA((CHUNKS + 1,)),
        ],
        compiler_params=pltpu.CompilerParams(vmem_limit_bytes=40 * 1024 * 1024),
        name="tail",
    )(rows, keys, values, before, weighting, fade, cosine, sine_part, bias, sink_logits,
      pltpu.with_memory_space_constraint(whole, pltpu.HBM))


def on_device(
    tokens,
    norm_gain,
    ret_query,
    ret_key,
    ret_value,
    log_decay,
    att_query,
    att_key,
    att_value,
    sink_logits,
    ret_out,
    att_out,
):
    core = lax.axis_index(CORE)
    tok_float = tokens.astype(jnp.float32)
    normed = (
        tok_float
        * lax.rsqrt(jnp.mean(tok_float * tok_float, axis=-1, keepdims=True) + epsilon)
        * norm_gain
    ).astype(jnp.bfloat16)
    weights = (ret_query, att_query, att_key, att_value)
    widths = [weight.shape[1] for weight in weights]
    whole = lax.all_gather(
        jnp.concatenate([*weights, ret_out.T, att_out.T], axis=1), SP, axis=0, tiled=True
    )
    head_weight = weight_of_head(ret_key, ret_value)
    own_rows = gathered_rows(normed, "tp")
    other_rows = core_swap(own_rows)
    tok_count = own_rows.shape[0]
    rim = shifted(own_rows[tok_count - WINDOW :], SP, 1)
    chip_rows = jnp.concatenate([own_rows, other_rows], axis=0)
    kv = jnp.dot(chip_rows, head_weight, preferred_element_type=jnp.float32).astype(jnp.bfloat16)
    kv = kv.reshape(2, tok_count, kv.shape[-1])
    decay_other = core_swap(log_decay)
    own_head = lax.dynamic_index_in_dim(log_decay, core, 0, keepdims=False)
    other_half = lax.dynamic_index_in_dim(decay_other, core, 0, keepdims=False)
    anchor = lax.axis_index(SP) * tok_count
    chip_anchor = lax.axis_index(ZY) * (2 * tok_count)
    keys, values, before = chain_of_head(
        in_core_order(kv[0], kv[1], 0), in_core_order(own_head, other_half, 0), chip_anchor
    )

    def heads_of_own_rows(value):
        halves = value.reshape(2, value.shape[0] // 2, *value.shape[1:])
        mine = lax.dynamic_index_in_dim(halves, core, 0, keepdims=False)
        theirs = lax.dynamic_index_in_dim(halves, 1 - core, 0, keepdims=False)
        return in_core_order(mine[None], core_swap(theirs)[None], 0)

    key_ret = heads_of_own_rows(keys)
    value_ret = heads_of_own_rows(values)
    before = heads_of_own_rows(before)

    input_width = sum(widths)
    partial = tail(
        jnp.concatenate([rim, own_rows], axis=0),
        key_ret,
        value_ret,
        before.astype(jnp.bfloat16),
        log_decay,
        sink_logits,
        whole,
        anchor,
        input_width,
    )
    mixed = summed_over_four(partial, "tp")
    return mixed.astype(jnp.bfloat16)


def solution(mesh):
    split = Mesh(mesh.devices.reshape(8, 8, 2, mesh.shape["tp"]), ("sp_0", "sp_1", "sp_2", "tp"))
    placed = (
        P(SP_TP, None),
        P(),
        P(SP, "tp"),
        P(SP, "tp"),
        P(SP, "tp"),
        P("tp", SP),
        P(SP, "tp"),
        P(SP, "tp"),
        P(SP, "tp"),
        P("tp"),
        P("tp", SP),
        P("tp", SP),
    )
    return jax.shard_map(
        on_device, mesh=split, in_specs=placed, out_specs=P(SP_TP, None), check_vma=False
    )
```

```python
import jax
import jax.numpy as jnp
from jax import lax
from jax.experimental import pallas as pl
from jax.experimental.pallas import tpu as pltpu
from jax.sharding import Mesh
from jax.sharding import PartitionSpec as P

RETAIN_KEY_SIZE = 128
V_DIM = 256
HEAD_DIM = 64
WINDOW = 128
BLOCK = 128
SP = ("sp_0", "sp_1", "sp_2")
SP_TP = ("sp_0", "sp_1", "sp_2", "tp")


epsilon = 1e-05
rope_base = 10000.0
masked_out = -1e30


def shifted(value, axis, steps):
    count = lax.axis_size(axis)
    initial, last = (max(0, -steps), min(count, count - steps))
    return lax.ppermute(value, axis, [(source, source + steps) for source in range(initial, last)])


def from_everyone(value, axis):
    size = lax.axis_size(axis)
    return lax.all_to_all(
        jnp.broadcast_to(value[None], (size, *value.shape)), axis, 0, 0, tiled=True
    )


def moved(value, axis, step):
    size = lax.axis_size(axis)
    return lax.ppermute(value, axis, [(k, (k + step) % size) for k in range(size)])


def cut_along(value, dim, size):
    before, after = (value.shape[:dim], value.shape[dim + 1 :])
    return jnp.moveaxis(value.reshape(*before, size, -1, *after), dim, 0)


def sent_and_summed(value, axis, dim):
    tiles = cut_along(value, dim, lax.axis_size(axis))
    arrived = lax.all_to_all(tiles, axis, split_axis=0, concat_axis=0, tiled=True)
    return arrived.astype(jnp.float32).sum(axis=0)


def rotate(values, positions):
    half_dim = values.shape[-1] // 2
    inverse = rope_base ** (-jnp.arange(half_dim, dtype=jnp.float32) / half_dim)
    angles = positions.astype(jnp.float32)[:, None] * inverse[None, :]
    cosine = jnp.cos(angles)[:, None, :]
    sine_part = jnp.sin(angles)[:, None, :]
    first_half = values[..., :half_dim].astype(jnp.float32)
    second_half = values[..., half_dim:].astype(jnp.float32)
    return jnp.concatenate(
        [
            first_half * cosine - second_half * sine_part,
            second_half * cosine + first_half * sine_part,
        ],
        axis=-1,
    )


ZY = ("sp_0", "sp_1")
CORE = "sp_2"


def core_swap(value):
    return lax.ppermute(value, CORE, [(0, 1), (1, 0)])


def in_core_order(own, other, axis):
    first = lax.axis_index(CORE) == 0
    return jnp.concatenate(
        [jnp.where(first, own, other), jnp.where(first, other, own)], axis=axis
    )


def prefix_body(parts_ref, out_ref):
    count = parts_ref.shape[0]
    carried = jnp.zeros(out_ref.shape[1:], jnp.float32)
    fades = [jnp.exp(parts_ref[k, 2:3]) for k in range(count)]
    for k in range(count):
        out_ref[k] = carried
        carried = carried * fades[k] + parts_ref[k, :2]


def states_body(arrived_ref, contrib_ref, fade_ref, core_ref, mine_ref, theirs_ref, state_ref):
    rows = arrived_ref.shape[1]
    for k in range(arrived_ref.shape[0]):
        state_ref[k * rows : (k + 1) * rows] = arrived_ref[k]
    blocks = contrib_ref.shape[0]
    here = blocks // 2
    state = state_ref[...]
    for n in range(blocks):
        rounded = state.astype(jnp.bfloat16)

        @pl.when(core_ref[0] == n // here)
        def _():
            mine_ref[n % here] = rounded

        @pl.when(core_ref[0] != n // here)
        def _():
            theirs_ref[n % here] = rounded

        if n + 1 < blocks:
            state = state * fade_ref[n] + contrib_ref[n]


def states(arrived, contrib, fades):
    half = jax.ShapeDtypeStruct((contrib.shape[0] // 2, *contrib.shape[1:]), jnp.bfloat16)
    vmem = pl.BlockSpec(memory_space=pltpu.VMEM)
    smem = pl.BlockSpec(memory_space=pltpu.SMEM)
    return pl.pallas_call(
        states_body,
        out_shape=(half, half),
        in_specs=[vmem, vmem, smem, smem],
        out_specs=(vmem, vmem),
        scratch_shapes=[pltpu.VMEM(contrib.shape[1:], jnp.float32)],
        name="states",
    )(arrived, contrib, fades, lax.axis_index(CORE).reshape(1))


def state_before(total, log_total):
    count = lax.axis_size(ZY)
    slices = total.reshape(count, 2, V_DIM)
    marks = jnp.broadcast_to(log_total, (count, 1, V_DIM))
    sent = jnp.concatenate([slices, marks], axis=1)
    arrived = lax.all_to_all(sent, ZY, 0, 0, tiled=True)
    prefix = pl.pallas_call(
        prefix_body, out_shape=jax.ShapeDtypeStruct((count, 2, V_DIM), jnp.float32)
    )(arrived)
    return lax.all_to_all(prefix, ZY, 0, 0, tiled=True)


def columns_of_head(ret_key, ret_value, head):
    return jnp.concatenate(
        [
            lax.dynamic_slice_in_dim(ret_key, head * RETAIN_KEY_SIZE, RETAIN_KEY_SIZE, 1),
            lax.dynamic_slice_in_dim(ret_value, head * V_DIM, V_DIM, 1),
        ],
        axis=1,
    )


def weight_of_head(ret_key, ret_value):
    core = lax.axis_index(CORE)
    mine = columns_of_head(ret_key, ret_value, core)
    theirs = core_swap(columns_of_head(ret_key, ret_value, 1 - core))
    block = in_core_order(mine, theirs, 0)
    arrived = from_everyone(block, "sp_1")
    part = arrived.reshape(-1, block.shape[-1])
    return ring_gathered(part, "sp_0")


def ring_gathered(part, axis):
    size = lax.axis_size(axis)
    here = lax.axis_index(axis)
    rows = part.shape[0]
    whole = jnp.zeros((size * rows, part.shape[1]), part.dtype)

    def put(whole, value, owner, offset=0):
        return lax.dynamic_update_slice_in_dim(whole, value, owner % size * rows + offset, 0)

    whole = put(whole, part, here)
    up = down = part
    for step in range(1, size // 2):
        up = moved(up, axis, 1)
        down = moved(down, axis, -1)
        whole = put(whole, up, here - step + size)
        whole = put(whole, down, here + step)
    half = rows // 2
    up = moved(up[:half], axis, 1)
    down = moved(down[half:], axis, -1)
    whole = put(whole, up, here + size // 2)
    return put(whole, down, here + size // 2, half)


def gathered_rows(value, axis):
    size = lax.axis_size(axis)
    here = lax.axis_index(axis)
    rows = value.shape[0]
    whole = jnp.zeros((size * rows, value.shape[1]), value.dtype)
    whole = lax.dynamic_update_slice_in_dim(whole, value, here * rows, 0)
    for step in range(1, size):
        piece = moved(value, axis, step)
        whole = lax.dynamic_update_slice_in_dim(
            whole, piece, (here - step + size) % size * rows, 0
        )
    return whole


def chain_of_head(kv, log_decay, anchor):
    length = kv.shape[0]
    blocks = length // BLOCK
    positions = anchor + jnp.arange(length, dtype=jnp.int32)
    keys = (
        rotate(kv[:, None, :RETAIN_KEY_SIZE], positions)[:, 0] * RETAIN_KEY_SIZE ** (-0.5)
    ).astype(jnp.bfloat16)
    values = kv[:, RETAIN_KEY_SIZE:]
    running = jnp.cumsum(log_decay.reshape(blocks, BLOCK), axis=-1)
    closing = running[:, -1]
    faded = (
        keys.reshape(blocks, BLOCK, -1).astype(jnp.float32)
        * jnp.exp(closing[:, None] - running)[..., None]
    ).astype(jnp.bfloat16)
    contrib = jnp.einsum(
        "njd,njv->ndv", faded, values.reshape(blocks, BLOCK, -1), preferred_element_type=jnp.float32
    )
    total = contrib[0]
    for n in range(1, blocks):
        total = total * jnp.exp(closing[n]) + contrib[n]
    arrived = state_before(total, jnp.sum(closing))
    mine, theirs = states(arrived, contrib, jnp.exp(closing))
    return keys, values, mine, core_swap(theirs)


CHUNKS = 4


def tail_body(
    rows_ref, key_ref, value_ref, own_ref, other_ref, running_ref, column_ref, cos_ref, sin_ref,
    sink_ref, place_ref, whole_ref, out_ref, win_ref, wout_ref, ret_ref, att_ref, sems,
):
    width, in_width = (rows_ref.shape[1], win_ref.shape[1])
    length = out_ref.shape[0]
    step = width // CHUNKS
    copies = [
        pltpu.make_async_copy(
            whole_ref.at[pl.ds(k * step, step), pl.ds(0, in_width)],
            win_ref.at[pl.ds(k * step, step)],
            sems.at[k],
        )
        for k in range(CHUNKS)
    ]
    copies.append(
        pltpu.make_async_copy(
            whole_ref.at[:, pl.ds(in_width, wout_ref.shape[1])], wout_ref, sems.at[CHUNKS]
        )
    )
    for copy in copies:
        copy.start()
    total = None
    for k in range(CHUNKS):
        copies[k].wait()
        part = jnp.dot(
            rows_ref[:, k * step : (k + 1) * step],
            win_ref[k * step : (k + 1) * step],
            preferred_element_type=jnp.float32,
        )
        total = part if total is None else total + part
    projected = total.astype(jnp.bfloat16)
    heads, blocks = (key_ref.shape[0], own_ref.shape[0])
    here = lax.broadcasted_iota(jnp.int32, (BLOCK, BLOCK), 0)
    causal_mask = here >= lax.broadcasted_iota(jnp.int32, (BLOCK, BLOCK), 1)
    core = place_ref[0]
    rim = rows_ref.shape[0] - length
    cosine = cos_ref[...]
    sine_part = sin_ref[...]
    contract_last = (((1,), (1,)), ((), ()))
    for h in range(heads):
        query = projected[rim:, h * RETAIN_KEY_SIZE : (h + 1) * RETAIN_KEY_SIZE].astype(jnp.float32)
        turned = pltpu.roll(query, RETAIN_KEY_SIZE // 2, 1)
        query = (query * cosine + turned * sine_part).astype(jnp.bfloat16)
        faded = (query.astype(jnp.float32) * jnp.exp(column_ref[h])).astype(jnp.bfloat16)
        for n in range(blocks):
            part = slice(n * BLOCK, (n + 1) * BLOCK)
            scores = lax.dot_general(
                query[part], key_ref[h, part], contract_last, preferred_element_type=jnp.float32
            )
            within = column_ref[h, part] - running_ref[h, n : n + 1]
            weighting = jnp.where(causal_mask, jnp.exp(jnp.minimum(within, 0.0)), 0.0)
            scores = (scores * weighting).astype(jnp.bfloat16)
            before = jnp.where(core == h, own_ref[n], other_ref[n])
            mixed = jnp.dot(scores, value_ref[h, part], preferred_element_type=jnp.float32)
            mixed = mixed + jnp.dot(faded[part], before, preferred_element_type=jnp.float32)
            mixed = mixed * lax.rsqrt(jnp.mean(mixed * mixed, axis=-1, keepdims=True) + epsilon)
            ret_ref[part, h * V_DIM : (h + 1) * V_DIM] = mixed.astype(jnp.bfloat16)
    first = heads * RETAIN_KEY_SIZE
    group = sink_ref.shape[0]
    keys_at = first + group * HEAD_DIM
    keys = projected[:, keys_at : keys_at + HEAD_DIM]
    values = projected[:, keys_at + HEAD_DIM : keys_at + 2 * HEAD_DIM]
    for n in range(length // WINDOW):
        seen = slice(n * WINDOW, (n + 2) * WINDOW)
        ahead = lax.broadcasted_iota(jnp.int32, (WINDOW, 2 * WINDOW), 1)
        offset = ahead - lax.broadcasted_iota(jnp.int32, (WINDOW, 2 * WINDOW), 0)
        there = ahead + (place_ref[1] + (n - 1) * WINDOW) >= 0
        allowed = (offset > 0) & (offset <= WINDOW) & there
        for g in range(0, group, 2):
            pair = []
            for k in (g, g + 1):
                at = first + k * HEAD_DIM
                query = projected[rim + n * WINDOW : rim + (n + 1) * WINDOW, at : at + HEAD_DIM]
                scores = lax.dot_general(
                    query, keys[seen], contract_last, preferred_element_type=jnp.float32
                )
                scores = jnp.where(allowed, scores * HEAD_DIM ** (-0.5), masked_out)
                sink = jnp.full((WINDOW, 1), sink_ref[k], jnp.float32)
                highest = jnp.maximum(jnp.max(scores, axis=-1, keepdims=True), sink)
                lifted = jnp.exp(scores - highest)
                below = jnp.sum(lifted, axis=-1, keepdims=True) + jnp.exp(sink - highest)
                found = jnp.dot(
                    lifted.astype(jnp.bfloat16), values[seen], preferred_element_type=jnp.float32
                )
                pair.append(found / below)
            att_ref[n * WINDOW : (n + 1) * WINDOW, g * HEAD_DIM : (g + 2) * HEAD_DIM] = (
                jnp.concatenate(pair, axis=1).astype(jnp.bfloat16)
            )
    copies[CHUNKS].wait()
    half = ret_ref.shape[1]
    result = lax.dot_general(
        ret_ref[...], wout_ref[:, :half], contract_last, preferred_element_type=jnp.float32
    ) + lax.dot_general(
        att_ref[...], wout_ref[:, half:], contract_last, preferred_element_type=jnp.float32
    )
    out_ref[...] = result.astype(jnp.bfloat16)


def tail(rows, keys, values, own, other, core, log_decay, sink_logits, whole, anchor, in_width):
    length = keys.shape[1]
    heads, blocks = (keys.shape[0], own.shape[0])
    running = jnp.cumsum(log_decay.reshape(heads, blocks, BLOCK), axis=-1)
    column = running.reshape(heads, length, 1)
    half_dim = RETAIN_KEY_SIZE // 2
    inverse = rope_base ** (-jnp.arange(half_dim, dtype=jnp.float32) / half_dim)
    positions = anchor + jnp.arange(length, dtype=jnp.int32)
    angles = positions.astype(jnp.float32)[:, None] * inverse[None, :]
    cosine = jnp.concatenate([jnp.cos(angles)] * 2, axis=1)
    sine_part = jnp.concatenate([-jnp.sin(angles), jnp.sin(angles)], axis=1)
    place = jnp.stack([core, anchor]).astype(jnp.int32)
    out_width = whole.shape[1] - in_width
    features = rows.shape[1]
    columns = whole.shape[0]
    vmem = pl.BlockSpec(memory_space=pltpu.VMEM)
    return pl.pallas_call(
        tail_body,
        out_shape=jax.ShapeDtypeStruct((length, columns), jnp.bfloat16),
        in_specs=[vmem] * 9
        + [pl.BlockSpec(memory_space=pltpu.SMEM)] * 2
        + [pl.BlockSpec(memory_space=pltpu.HBM)],
        out_specs=vmem,
        scratch_shapes=[
            pltpu.VMEM((features, in_width), jnp.bfloat16),
            pltpu.VMEM((columns, out_width), jnp.bfloat16),
            pltpu.VMEM((length, heads * V_DIM), jnp.bfloat16),
            pltpu.VMEM((length, sink_logits.shape[0] * HEAD_DIM), jnp.bfloat16),
            pltpu.SemaphoreType.DMA((CHUNKS + 1,)),
        ],
        compiler_params=pltpu.CompilerParams(vmem_limit_bytes=40 * 1024 * 1024),
        name="tail",
    )(
        rows, keys, values, own, other, running, column, cosine, sine_part, sink_logits, place,
        pltpu.with_memory_space_constraint(whole, pltpu.HBM),
    )


def on_device(
    tokens,
    norm_gain,
    ret_query,
    ret_key,
    ret_value,
    log_decay,
    att_query,
    att_key,
    att_value,
    sink_logits,
    ret_out,
    att_out,
):
    core = lax.axis_index(CORE)
    tok_float = tokens.astype(jnp.float32)
    normed = (
        tok_float
        * lax.rsqrt(jnp.mean(tok_float * tok_float, axis=-1, keepdims=True) + epsilon)
        * norm_gain
    ).astype(jnp.bfloat16)
    normed = lax.optimization_barrier(normed)
    weights = (ret_query, att_query, att_key, att_value)
    widths = [weight.shape[1] for weight in weights]
    whole = lax.all_gather(
        jnp.concatenate([*weights, ret_out.T, att_out.T], axis=1), SP, axis=0, tiled=True
    )
    head_weight = weight_of_head(ret_key, ret_value)
    own_rows = gathered_rows(normed, "tp")
    other_rows = core_swap(own_rows)
    tok_count = own_rows.shape[0]
    rim = shifted(own_rows[tok_count - WINDOW :], SP, 1)
    chip_rows = jnp.concatenate([own_rows, other_rows], axis=0)
    kv = jnp.dot(chip_rows, head_weight, preferred_element_type=jnp.float32).astype(jnp.bfloat16)
    kv = kv.reshape(2, tok_count, kv.shape[-1])
    decay_other = core_swap(log_decay)
    own_head = lax.dynamic_index_in_dim(log_decay, core, 0, keepdims=False)
    other_half = lax.dynamic_index_in_dim(decay_other, core, 0, keepdims=False)
    anchor = lax.axis_index(SP) * tok_count
    chip_anchor = lax.axis_index(ZY) * (2 * tok_count)
    keys, values, state_own, state_other = chain_of_head(
        in_core_order(kv[0], kv[1], 0), in_core_order(own_head, other_half, 0), chip_anchor
    )

    def heads_of_own_rows(value):
        halves = value.reshape(2, value.shape[0] // 2, *value.shape[1:])
        mine = lax.dynamic_index_in_dim(halves, core, 0, keepdims=False)
        theirs = lax.dynamic_index_in_dim(halves, 1 - core, 0, keepdims=False)
        return in_core_order(mine[None], core_swap(theirs)[None], 0)

    key_ret = heads_of_own_rows(keys)
    value_ret = heads_of_own_rows(values)

    input_width = sum(widths)
    partial = tail(
        jnp.concatenate([rim, own_rows], axis=0),
        key_ret,
        value_ret,
        state_own,
        state_other,
        core,
        log_decay,
        sink_logits,
        whole,
        anchor,
        input_width,
    )
    mixed = sent_and_summed(partial, "tp", 0)
    return mixed.astype(jnp.bfloat16)


def solution(mesh):
    split = Mesh(mesh.devices.reshape(8, 8, 2, mesh.shape["tp"]), ("sp_0", "sp_1", "sp_2", "tp"))
    placed = (
        P(SP_TP, None),
        P(),
        P(SP, "tp"),
        P(SP, "tp"),
        P(SP, "tp"),
        P("tp", SP),
        P(SP, "tp"),
        P(SP, "tp"),
        P(SP, "tp"),
        P("tp"),
        P("tp", SP),
        P("tp", SP),
    )
    return jax.shard_map(
        on_device, mesh=split, in_specs=placed, out_specs=P(SP_TP, None), check_vma=False
    )
```

```python
import jax
import jax.numpy as jnp
from jax import lax
from jax.experimental import pallas as pl
from jax.experimental.pallas import tpu as pltpu
from jax.sharding import Mesh
from jax.sharding import PartitionSpec as P

RETAIN_KEY_SIZE = 128
V_DIM = 256
HEAD_DIM = 64
WINDOW = 128
BLOCK = 128
SP = ("sp_0", "sp_1", "sp_2")
SP_TP = ("sp_0", "sp_1", "sp_2", "tp")


epsilon = 1e-05
rope_base = 10000.0
masked_out = -1e30


def shifted(value, axis, steps):
    count = lax.axis_size(axis)
    initial, last = (max(0, -steps), min(count, count - steps))
    return lax.ppermute(value, axis, [(source, source + steps) for source in range(initial, last)])


def from_everyone(value, axis):
    size = lax.axis_size(axis)
    return lax.all_to_all(
        jnp.broadcast_to(value[None], (size, *value.shape)), axis, 0, 0, tiled=True
    )


def moved(value, axis, step):
    size = lax.axis_size(axis)
    return lax.ppermute(value, axis, [(k, (k + step) % size) for k in range(size)])


def cut_along(value, dim, size):
    before, after = (value.shape[:dim], value.shape[dim + 1 :])
    return jnp.moveaxis(value.reshape(*before, size, -1, *after), dim, 0)


def sent_and_summed(value, axis, dim):
    tiles = cut_along(value, dim, lax.axis_size(axis))
    arrived = lax.all_to_all(tiles, axis, split_axis=0, concat_axis=0, tiled=True)
    return arrived.astype(jnp.float32).sum(axis=0)


def rotate(values, positions):
    half_dim = values.shape[-1] // 2
    inverse = rope_base ** (-jnp.arange(half_dim, dtype=jnp.float32) / half_dim)
    angles = positions.astype(jnp.float32)[:, None] * inverse[None, :]
    cosine = jnp.cos(angles)[:, None, :]
    sine_part = jnp.sin(angles)[:, None, :]
    first_half = values[..., :half_dim].astype(jnp.float32)
    second_half = values[..., half_dim:].astype(jnp.float32)
    return jnp.concatenate(
        [
            first_half * cosine - second_half * sine_part,
            second_half * cosine + first_half * sine_part,
        ],
        axis=-1,
    )


ZY = ("sp_0", "sp_1")
CORE = "sp_2"


def core_swap(value):
    return lax.ppermute(value, CORE, [(0, 1), (1, 0)])


def in_core_order(own, other, axis):
    first = lax.axis_index(CORE) == 0
    return jnp.concatenate(
        [jnp.where(first, own, other), jnp.where(first, other, own)], axis=axis
    )


def prefix_body(parts_ref, out_ref):
    count = parts_ref.shape[0]
    carried = jnp.zeros(out_ref.shape[1:], jnp.float32)
    fades = [jnp.exp(parts_ref[k, 2:3]) for k in range(count)]
    for k in range(count):
        out_ref[k] = carried
        carried = carried * fades[k] + parts_ref[k, :2]


def states_body(arrived_ref, contrib_ref, fade_ref, core_ref, mine_ref, theirs_ref, state_ref):
    rows = arrived_ref.shape[1]
    for k in range(arrived_ref.shape[0]):
        state_ref[k * rows : (k + 1) * rows] = arrived_ref[k]
    blocks = contrib_ref.shape[0]
    here = blocks // 2
    state = state_ref[...]
    for n in range(blocks):
        rounded = state.astype(jnp.bfloat16)

        @pl.when(core_ref[0] == n // here)
        def _():
            mine_ref[n % here] = rounded

        @pl.when(core_ref[0] != n // here)
        def _():
            theirs_ref[n % here] = rounded

        if n + 1 < blocks:
            state = state * fade_ref[n] + contrib_ref[n]


def states(arrived, contrib, fades):
    half = jax.ShapeDtypeStruct((contrib.shape[0] // 2, *contrib.shape[1:]), jnp.bfloat16)
    vmem = pl.BlockSpec(memory_space=pltpu.VMEM)
    smem = pl.BlockSpec(memory_space=pltpu.SMEM)
    return pl.pallas_call(
        states_body,
        out_shape=(half, half),
        in_specs=[vmem, vmem, smem, smem],
        out_specs=(vmem, vmem),
        scratch_shapes=[pltpu.VMEM(contrib.shape[1:], jnp.float32)],
        compiler_params=pltpu.CompilerParams(vmem_limit_bytes=8 * 1024 * 1024),
        name="states",
    )(arrived, contrib, fades, lax.axis_index(CORE).reshape(1))


def state_before(total, log_total):
    count = lax.axis_size(ZY)
    slices = total.reshape(count, 2, V_DIM)
    marks = jnp.broadcast_to(log_total, (count, 1, V_DIM))
    sent = jnp.concatenate([slices, marks], axis=1)
    arrived = lax.all_to_all(sent, ZY, 0, 0, tiled=True)
    prefix = pl.pallas_call(
        prefix_body,
        out_shape=jax.ShapeDtypeStruct((count, 2, V_DIM), jnp.float32),
        compiler_params=pltpu.CompilerParams(vmem_limit_bytes=8 * 1024 * 1024),
    )(arrived)
    return lax.all_to_all(prefix, ZY, 0, 0, tiled=True)


def columns_of_head(ret_key, ret_value, head):
    return jnp.concatenate(
        [
            lax.dynamic_slice_in_dim(ret_key, head * RETAIN_KEY_SIZE, RETAIN_KEY_SIZE, 1),
            lax.dynamic_slice_in_dim(ret_value, head * V_DIM, V_DIM, 1),
        ],
        axis=1,
    )


def weight_of_head(ret_key, ret_value):
    core = lax.axis_index(CORE)
    mine = columns_of_head(ret_key, ret_value, core)
    theirs = core_swap(columns_of_head(ret_key, ret_value, 1 - core))
    block = in_core_order(mine, theirs, 0)
    arrived = from_everyone(block, "sp_1")
    part = arrived.reshape(-1, block.shape[-1])
    return ring_gathered(part, "sp_0")


def ring_gathered(part, axis):
    size = lax.axis_size(axis)
    here = lax.axis_index(axis)
    rows = part.shape[0]
    whole = jnp.zeros((size * rows, part.shape[1]), part.dtype)

    def put(whole, value, owner, offset=0):
        return lax.dynamic_update_slice_in_dim(whole, value, owner % size * rows + offset, 0)

    whole = put(whole, part, here)
    up = down = part
    for step in range(1, size // 2):
        up = moved(up, axis, 1)
        down = moved(down, axis, -1)
        whole = put(whole, up, here - step + size)
        whole = put(whole, down, here + step)
    half = rows // 2
    up = moved(up[:half], axis, 1)
    down = moved(down[half:], axis, -1)
    whole = put(whole, up, here + size // 2)
    return put(whole, down, here + size // 2, half)


def chain_of_head(kv, log_decay, anchor):
    length = kv.shape[0]
    blocks = length // BLOCK
    positions = anchor + jnp.arange(length, dtype=jnp.int32)
    keys = (
        rotate(kv[:, None, :RETAIN_KEY_SIZE], positions)[:, 0] * RETAIN_KEY_SIZE ** (-0.5)
    ).astype(jnp.bfloat16)
    values = kv[:, RETAIN_KEY_SIZE:]
    running = jnp.cumsum(log_decay.reshape(blocks, BLOCK), axis=-1)
    closing = running[:, -1]
    fades = jnp.exp(closing)
    key_fades = jnp.exp(closing[:, None] - running)
    log_total = jnp.sum(closing)
    faded = (
        keys.reshape(blocks, BLOCK, -1).astype(jnp.float32)
        * key_fades[..., None]
    ).astype(jnp.bfloat16)
    contrib = jnp.einsum(
        "njd,njv->ndv", faded, values.reshape(blocks, BLOCK, -1), preferred_element_type=jnp.float32
    )
    total = contrib[0]
    for n in range(1, blocks):
        total = total * fades[n] + contrib[n]
    arrived = state_before(total, log_total)
    mine, theirs = states(arrived, contrib, fades)
    return keys, values, mine, core_swap(theirs)


CHUNKS = 4


def front_body(
    rows_ref, key_ref, value_ref, running_ref, column_ref, cos_ref, sin_ref, sink_ref, place_ref,
    whole_ref, inner_ref, faded_ref, part_ref, win_ref, wout_ref, att_ref, sems,
):
    width, in_width = (rows_ref.shape[1], win_ref.shape[1])
    length = part_ref.shape[0]
    step = width // CHUNKS
    copies = [
        pltpu.make_async_copy(
            whole_ref.at[pl.ds(k * step, step), pl.ds(0, in_width)],
            win_ref.at[pl.ds(k * step, step)],
            sems.at[k],
        )
        for k in range(CHUNKS)
    ]
    copies.append(
        pltpu.make_async_copy(
            whole_ref.at[:, pl.ds(whole_ref.shape[1] - wout_ref.shape[1], wout_ref.shape[1])],
            wout_ref,
            sems.at[CHUNKS],
        )
    )
    for copy in copies:
        copy.start()
    total = None
    for k in range(CHUNKS):
        copies[k].wait()
        part = jnp.dot(
            rows_ref[:, k * step : (k + 1) * step],
            win_ref[k * step : (k + 1) * step],
            preferred_element_type=jnp.float32,
        )
        total = part if total is None else total + part
    projected = total.astype(jnp.bfloat16)
    heads, blocks = (key_ref.shape[0], length // BLOCK)
    here = lax.broadcasted_iota(jnp.int32, (BLOCK, BLOCK), 0)
    causal_mask = here >= lax.broadcasted_iota(jnp.int32, (BLOCK, BLOCK), 1)
    rim = rows_ref.shape[0] - length
    cosine = cos_ref[...]
    sine_part = sin_ref[...]
    contract_last = (((1,), (1,)), ((), ()))
    for h in range(heads):
        query = projected[rim:, h * RETAIN_KEY_SIZE : (h + 1) * RETAIN_KEY_SIZE].astype(jnp.float32)
        turned = pltpu.roll(query, RETAIN_KEY_SIZE // 2, 1)
        query = (query * cosine + turned * sine_part).astype(jnp.bfloat16)
        faded = query.astype(jnp.float32) * jnp.exp(column_ref[h])
        faded_ref[:, h * RETAIN_KEY_SIZE : (h + 1) * RETAIN_KEY_SIZE] = faded.astype(jnp.bfloat16)
        for n in range(blocks):
            part = slice(n * BLOCK, (n + 1) * BLOCK)
            scores = lax.dot_general(
                query[part], key_ref[h, part], contract_last, preferred_element_type=jnp.float32
            )
            within = column_ref[h, part] - running_ref[h, n : n + 1]
            weighting = jnp.where(causal_mask, jnp.exp(jnp.minimum(within, 0.0)), 0.0)
            scores = (scores * weighting).astype(jnp.bfloat16)
            inner_ref[part, h * V_DIM : (h + 1) * V_DIM] = jnp.dot(
                scores, value_ref[h, part], preferred_element_type=jnp.float32
            )
    first = heads * RETAIN_KEY_SIZE
    group = sink_ref.shape[0]
    keys_at = first + group * HEAD_DIM
    keys = projected[:, keys_at : keys_at + HEAD_DIM]
    values = projected[:, keys_at + HEAD_DIM : keys_at + 2 * HEAD_DIM]
    for n in range(length // WINDOW):
        seen = slice(n * WINDOW, (n + 2) * WINDOW)
        ahead = lax.broadcasted_iota(jnp.int32, (WINDOW, 2 * WINDOW), 1)
        offset = ahead - lax.broadcasted_iota(jnp.int32, (WINDOW, 2 * WINDOW), 0)
        there = ahead + (place_ref[0] + (n - 1) * WINDOW) >= 0
        allowed = (offset > 0) & (offset <= WINDOW) & there
        for g in range(0, group, 2):
            pair = []
            for k in (g, g + 1):
                at = first + k * HEAD_DIM
                query = projected[rim + n * WINDOW : rim + (n + 1) * WINDOW, at : at + HEAD_DIM]
                scores = lax.dot_general(
                    query, keys[seen], contract_last, preferred_element_type=jnp.float32
                )
                scores = jnp.where(allowed, scores * HEAD_DIM ** (-0.5), masked_out)
                sink = jnp.full((WINDOW, 1), sink_ref[k], jnp.float32)
                highest = jnp.maximum(jnp.max(scores, axis=-1, keepdims=True), sink)
                lifted = jnp.exp(scores - highest)
                below = jnp.sum(lifted, axis=-1, keepdims=True) + jnp.exp(sink - highest)
                found = jnp.dot(
                    lifted.astype(jnp.bfloat16), values[seen], preferred_element_type=jnp.float32
                )
                pair.append(found / below)
            att_ref[n * WINDOW : (n + 1) * WINDOW, g * HEAD_DIM : (g + 2) * HEAD_DIM] = (
                jnp.concatenate(pair, axis=1).astype(jnp.bfloat16)
            )
    copies[CHUNKS].wait()
    part_ref[...] = lax.dot_general(
        att_ref[...], wout_ref[...], contract_last, preferred_element_type=jnp.float32
    )


def back_body(
    inner_ref, faded_ref, part_ref, own_ref, other_ref, place_ref, whole_ref, out_ref, wout_ref,
    ret_ref, sem,
):
    width = wout_ref.shape[1]
    start = whole_ref.shape[1] - 2 * width
    copy = pltpu.make_async_copy(whole_ref.at[:, pl.ds(start, width)], wout_ref, sem)
    copy.start()
    core = place_ref[0]
    for h in range(ret_ref.shape[1] // V_DIM):
        columns = slice(h * V_DIM, (h + 1) * V_DIM)
        depth = slice(h * RETAIN_KEY_SIZE, (h + 1) * RETAIN_KEY_SIZE)
        for n in range(own_ref.shape[0]):
            part = slice(n * BLOCK, (n + 1) * BLOCK)
            before = jnp.where(core == h, own_ref[n], other_ref[n])
            mixed = inner_ref[part, columns] + jnp.dot(
                faded_ref[part, depth], before, preferred_element_type=jnp.float32
            )
            mixed = mixed * lax.rsqrt(jnp.mean(mixed * mixed, axis=-1, keepdims=True) + epsilon)
            ret_ref[part, columns] = mixed.astype(jnp.bfloat16)
    copy.wait()
    result = part_ref[...] + lax.dot_general(
        ret_ref[...], wout_ref[...], (((1,), (1,)), ((), ())), preferred_element_type=jnp.float32
    )
    out_ref[...] = result.astype(jnp.bfloat16)


def tail(rows, keys, values, own, other, core, log_decay, sink_logits, whole, anchor, in_width):
    length = keys.shape[1]
    heads, blocks = (keys.shape[0], length // BLOCK)
    running = jnp.cumsum(log_decay.reshape(heads, blocks, BLOCK), axis=-1)
    column = running.reshape(heads, length, 1)
    half_dim = RETAIN_KEY_SIZE // 2
    inverse = rope_base ** (-jnp.arange(half_dim, dtype=jnp.float32) / half_dim)
    positions = anchor + jnp.arange(length, dtype=jnp.int32)
    angles = positions.astype(jnp.float32)[:, None] * inverse[None, :]
    cosine = jnp.concatenate([jnp.cos(angles)] * 2, axis=1)
    sine_part = jnp.concatenate([-jnp.sin(angles), jnp.sin(angles)], axis=1)
    half = (whole.shape[1] - in_width) // 2
    features = rows.shape[1]
    columns = whole.shape[0]
    vmem = pl.BlockSpec(memory_space=pltpu.VMEM)
    smem = pl.BlockSpec(memory_space=pltpu.SMEM)
    hbm = pl.BlockSpec(memory_space=pltpu.HBM)
    whole = pltpu.with_memory_space_constraint(whole, pltpu.HBM)
    inner, faded, part = pl.pallas_call(
        front_body,
        out_shape=(
            jax.ShapeDtypeStruct((length, heads * V_DIM), jnp.float32),
            jax.ShapeDtypeStruct((length, heads * RETAIN_KEY_SIZE), jnp.bfloat16),
            jax.ShapeDtypeStruct((length, columns), jnp.float32),
        ),
        in_specs=[vmem] * 7 + [smem] * 2 + [hbm],
        out_specs=(vmem, vmem, vmem),
        scratch_shapes=[
            pltpu.VMEM((features, in_width), jnp.bfloat16),
            pltpu.VMEM((columns, half), jnp.bfloat16),
            pltpu.VMEM((length, half), jnp.bfloat16),
            pltpu.SemaphoreType.DMA((CHUNKS + 1,)),
        ],
        compiler_params=pltpu.CompilerParams(vmem_limit_bytes=24 * 1024 * 1024),
        name="front",
    )(
        rows, keys, values, running, column, cosine, sine_part, sink_logits,
        anchor.astype(jnp.int32).reshape(1), whole,
    )
    return pl.pallas_call(
        back_body,
        out_shape=jax.ShapeDtypeStruct((length, columns), jnp.bfloat16),
        in_specs=[vmem] * 5 + [smem, hbm],
        out_specs=vmem,
        scratch_shapes=[
            pltpu.VMEM((columns, half), jnp.bfloat16),
            pltpu.VMEM((length, heads * V_DIM), jnp.bfloat16),
            pltpu.SemaphoreType.DMA(()),
        ],
        compiler_params=pltpu.CompilerParams(vmem_limit_bytes=16 * 1024 * 1024),
        name="back",
    )(inner, faded, part, own, other, core.astype(jnp.int32).reshape(1), whole)


def on_device(
    tokens,
    norm_gain,
    ret_query,
    ret_key,
    ret_value,
    log_decay,
    att_query,
    att_key,
    att_value,
    sink_logits,
    ret_out,
    att_out,
):
    core = lax.axis_index(CORE)
    tok_float = tokens.astype(jnp.float32)
    normed = (
        tok_float
        * lax.rsqrt(jnp.mean(tok_float * tok_float, axis=-1, keepdims=True) + epsilon)
        * norm_gain
    ).astype(jnp.bfloat16)
    normed = lax.optimization_barrier(normed)
    weights = (ret_query, att_query, att_key, att_value)
    widths = [weight.shape[1] for weight in weights]
    whole = lax.all_gather(
        jnp.concatenate([*weights, ret_out.T, att_out.T], axis=1), SP, axis=0, tiled=True
    )
    head_weight = weight_of_head(ret_key, ret_value)
    own_rows = from_everyone(normed, "tp").reshape(-1, normed.shape[1])
    other_rows = core_swap(own_rows)
    tok_count = own_rows.shape[0]
    rim = shifted(own_rows[tok_count - WINDOW :], SP, 1)
    chip_rows = jnp.concatenate([own_rows, other_rows], axis=0)
    kv = jnp.dot(chip_rows, head_weight, preferred_element_type=jnp.float32).astype(jnp.bfloat16)
    kv = kv.reshape(2, tok_count, kv.shape[-1])
    decay_other = core_swap(log_decay)
    own_head = lax.dynamic_index_in_dim(log_decay, core, 0, keepdims=False)
    other_half = lax.dynamic_index_in_dim(decay_other, core, 0, keepdims=False)
    anchor = lax.axis_index(SP) * tok_count
    chip_anchor = lax.axis_index(ZY) * (2 * tok_count)
    keys, values, state_own, state_other = chain_of_head(
        in_core_order(kv[0], kv[1], 0), in_core_order(own_head, other_half, 0), chip_anchor
    )

    def heads_of_own_rows(value):
        halves = value.reshape(2, value.shape[0] // 2, *value.shape[1:])
        mine = lax.dynamic_index_in_dim(halves, core, 0, keepdims=False)
        theirs = lax.dynamic_index_in_dim(halves, 1 - core, 0, keepdims=False)
        return in_core_order(mine[None], core_swap(theirs)[None], 0)

    key_ret = heads_of_own_rows(keys)
    value_ret = heads_of_own_rows(values)

    input_width = sum(widths)
    partial = tail(
        jnp.concatenate([rim, own_rows], axis=0),
        key_ret,
        value_ret,
        state_own,
        state_other,
        core,
        log_decay,
        sink_logits,
        whole,
        anchor,
        input_width,
    )
    mixed = sent_and_summed(partial, "tp", 0)
    return mixed.astype(jnp.bfloat16)


def solution(mesh):
    split = Mesh(mesh.devices.reshape(8, 8, 2, mesh.shape["tp"]), ("sp_0", "sp_1", "sp_2", "tp"))
    placed = (
        P(SP_TP, None),
        P(),
        P(SP, "tp"),
        P(SP, "tp"),
        P(SP, "tp"),
        P("tp", SP),
        P(SP, "tp"),
        P(SP, "tp"),
        P(SP, "tp"),
        P("tp"),
        P("tp", SP),
        P("tp", SP),
    )
    return jax.shard_map(
        on_device, mesh=split, in_specs=placed, out_specs=P(SP_TP, None), check_vma=False
    )
```
